256 devices in a mesh: sp: 16 (over y, x), tp: 16 (over z, core).
Axes of the slice: x: 4, y: 4, z: 8, core: 2. Of those that a mesh axis runs over, the one named last changes fastest.
Arguments:
- mix_in: bfloat16 [16384, 2048], P('sp', 'tp'), may hold values from -8 to 8
- gate_in: bfloat16 [16384, 2048], P('sp', 'tp'), may hold values from -6 to 6
- conv_w: float32 [4, 2048], P(None, 'tp'), may hold values from -3 to 3
- conv_b: float32 [2048], P('tp'), may hold values from -3 to 3
- decay_param: float32 [2, 2048], P(None, 'tp')
- recur_gate: float32 [2, 32, 64, 64], P(None, 'tp'), may hold values from -0.75 to 0.75
- recur_bias: float32 [2, 2048], P(None, 'tp'), may hold values from -4 to 4
- input_gate: float32 [2, 32, 64, 64], P(None, 'tp'), may hold values from -0.75 to 0.75
- input_bias: float32 [2, 2048], P(None, 'tp'), may hold values from -4 to 4
- residual: bfloat16 [16384, 2048], P(('sp', 'tp')), may hold values from -6 to 6
- out_proj: bfloat16 [2048, 2048], replicated, may hold values from -0.125 to 0.125
- norm_gain: float32 [3, 2048], replicated, may hold values from 0.1 to 1.9
- routes: int32 [16384, 2], P('sp'), may hold values from 0 to 15, all different within a row; in each aligned block of 64 rows (0 to 63, 64 to 127, ...) at most 16 rows name the same one
- route_wt: float32 [16384, 2], P('sp'), may hold values from 0.1 to 1
- exp_gate: bfloat16 [16, 2048, 1024], P('sp', None, 'tp'), may hold values from -0.125 to 0.125
- exp_up: bfloat16 [16, 2048, 1024], P('sp', None, 'tp'), may hold values from -0.125 to 0.125
- exp_down: bfloat16 [16, 1024, 2048], P('sp', 'tp'), may hold values from -0.1875 to 0.1875
Outputs:
- final: bfloat16 [16384, 2048], P(('sp', 'tp'))
The draws below stay inside these ranges and needn't reach their ends.
Inputs may be any that keep to these rules, and one draw needn't show every extreme that they name: `routes`: in each aligned block of 64 tokens (the rows of one device in the expert layer) no expert is named more than 16 times, and in some block some expert exactly 16 times; a token's 2 experts differ.
All inputs are finite; a program needn't handle non-finite values.
Results may differ from the reference program's by a relative error of at most 0.008.
Values may be sent and summed in bfloat16 or wider, within the bound.
A program may use at most 128 MiB of HBM per device.

```python
import math
import jax
import jax.numpy as jnp
import numpy as np
from jax import lax

D = 2048
WIDTH = 2048
HEAD = 64
FF = 1024
EXPERTS = 16
TOPK = 2
SEQ_DEV = 1024
HEADS = 32
SEQ = 16384
ROWS = 64
CAP = 16


def draw_decay_param(key, part):
    pick_key, slow_key, fast_key = jax.random.split(jax.random.fold_in(key, 17), 3)
    slow_share = 0.5
    chooser = jax.random.uniform(pick_key, (2, WIDTH), jnp.float32)
    slow_values = math.log(SEQ) + jax.random.uniform(slow_key, (2, WIDTH), jnp.float32, 0.7, 1.7)
    fast_values = jax.random.uniform(fast_key, (2, WIDTH), jnp.float32, 3.5, 5.0)
    return jnp.where(chooser < slow_share, slow_values, fast_values).astype(jnp.float32)


def draw_conv_w(key, part):
    tap_key = jax.random.fold_in(key, 31)
    values = jax.random.normal(tap_key, (4, WIDTH), jnp.float32)
    tap_scale = jnp.array([0.4, 0.4, 0.4, 1.2], jnp.float32)[:, None]
    return jnp.clip(values * tap_scale, -3.0, 3.0).astype(jnp.float32)


def draw_mix_in(key, part):
    value_key, scale_key, offset_key = jax.random.split(jax.random.fold_in(key, 23), 3)
    values = jax.random.normal(value_key, (SEQ, WIDTH), jnp.float32)
    spread = 0.8
    position = jnp.arange(SEQ, dtype=jnp.int32) % SEQ_DEV
    at_ends = jnp.logical_or(position < 2, position >= SEQ_DEV - 2)
    values = values * jnp.where(at_ends, 3.0, 1.0)[:, None]
    scales = jnp.exp(jax.random.uniform(scale_key, (SEQ // 64, 1, WIDTH), jnp.float32, -spread, spread))
    shaped = (values.reshape(SEQ // 64, 64, WIDTH) * scales).reshape(SEQ, WIDTH)
    offsets = jax.random.uniform(offset_key, (SEQ // SEQ_DEV, 1, WIDTH), jnp.float32, -1.5, 1.5)
    shifted = (shaped.reshape(SEQ // SEQ_DEV, SEQ_DEV, WIDTH) + offsets).reshape(SEQ, WIDTH)
    return jnp.clip(shifted, -8.0, 8.0).astype(jnp.bfloat16)


def level_of(key, extent, shards, smallest, high):
    loudness, own = 1.0, jax.random.fold_in(key, 6)
    for dim, parts in shards:
        draws = jnp.exp(jax.random.uniform(jax.random.fold_in(own, dim), (parts,), jnp.float32, smallest / len(shards), high / len(shards)))
        loudness = loudness * jnp.repeat(draws, extent[dim] // parts).reshape([-1 if axis == dim else 1 for axis in range(len(extent))])
    return loudness


def deal_out(stream_key, own, number, rows, count, top, reach, lean):
    sequence = jax.random.permutation(stream_key, count)
    crowded, ordinary = load_shares(count, rows * top, reach, lean, True), load_shares(count, rows * top, reach, lean, False)
    places = jnp.arange(count)

    def named(tallies, rotation):
        used = int((tallies > 0).sum())
        fixed = max(1, used // 4)
        passed = fixed + (places - fixed + rotation * (used - fixed)) % max(1, count - fixed)
        return jnp.zeros((count,), jnp.int32).at[sequence[jnp.where(places < fixed, places, passed)]].set(jnp.asarray(tallies, jnp.int32))

    tallies = jnp.where(number % 4 == 0, named(crowded, number // 4), named(ordinary, number - number // 4 - 1))
    mixed = jax.random.permutation(jax.random.fold_in(own, 3), count)
    source_of, sink = mixed[0:count // 2 * 2:2], mixed[1:count // 2 * 2:2]
    room = jnp.minimum(tallies[source_of] - 1, reach - tallies[sink]) // 2
    room = jnp.where((source_of == sequence[0]) | (sink == sequence[0]) | (tallies[sink] == 0), 0, jnp.maximum(room, 0))
    passed = jax.random.randint(jax.random.fold_in(own, 4), (count // 2,), 0, 1 << 20) % (room + 1)
    tallies = tallies.at[source_of].add(-passed).at[sink].add(passed)
    items = jnp.searchsorted(jnp.cumsum(tallies), jnp.arange(rows * top), side="right").astype(jnp.int32)
    table = items.reshape(top, rows).T
    table = table[jax.random.permutation(jax.random.fold_in(own, 1), rows)]
    rotation = jax.random.randint(jax.random.fold_in(own, 2), (rows, 1), 0, top)
    return jnp.take_along_axis(table, (jnp.arange(top)[None, :] + rotation) % top, axis=1)


def load_shares(count, total, most, lean, full):
    portions = [(1 << 20) // math.isqrt(standing ** lean) + 1 for standing in range(1, count + 1)]
    largest = most if full else min(most, max(-(-total // count), total * portions[0] // sum(portions)))
    least = 1 if total - largest >= count - 1 else 0
    holding, surplus = [largest] + [least] * (count - 1), total - largest - least * (count - 1)
    while surplus > 0:
        movable = [i for i in range(1, count) if holding[i] < largest] or [i for i in range(1, count) if holding[i] < most]
        pool, budget = sum([portions[i] for i in movable]), surplus
        for i in movable:
            more = min(most - holding[i], max(1, budget * portions[i] // pool), surplus)
            holding[i] = holding[i] + more
            surplus = surplus - more
    return np.array(holding)


def centred(stream_key, dims, deviation, limit, cuts=(), held_as=jnp.bfloat16):
    entries = jax.random.normal(stream_key, dims, jnp.float32) * deviation
    if len(cuts) > 0:
        entries = level_of(stream_key, dims, cuts, -0.22, 0.18) * entries
    return jnp.clip(entries, min=-limit, max=limit).astype(held_as)


def setup_inputs(seed: int = 0) -> dict:
    splits = jax.random.split(jax.random.key(seed), 18)
    mix_in = draw_mix_in(jax.random.fold_in(splits[17], 71), 0)
    gate_in = centred(splits[1], (SEQ, WIDTH), 1.0, 6.0, ((0, 16), (1, 16)))
    conv_w = draw_conv_w(jax.random.fold_in(splits[17], 71), 0)
    conv_b = centred(splits[3], (WIDTH,), 0.5, 3.0, ((0, 16),), jnp.float32)
    decay_param = draw_decay_param(jax.random.fold_in(splits[17], 71), 0)
    recur_gate = centred(splits[5], (2, HEADS, HEAD, HEAD), HEAD ** -0.5, 0.75, ((1, 16),), jnp.float32)
    recur_bias = centred(splits[6], (2, WIDTH), 1.0, 4.0, ((1, 16),), jnp.float32)
    input_gate = centred(splits[7], (2, HEADS, HEAD, HEAD), HEAD ** -0.5, 0.75, ((1, 16),), jnp.float32)
    input_bias = centred(splits[8], (2, WIDTH), 1.0, 4.0, ((1, 16),), jnp.float32)
    residual = centred(splits[9], (SEQ, D), 1.0, 6.0, ((0, 256),))
    out_proj = centred(splits[10], (WIDTH, D), WIDTH ** -0.5, 0.125)
    norm_gain = jnp.clip(1.0 + 0.18 * jax.random.normal(splits[11], (3, D), jnp.float32), 0.1, 1.9)
    routes_keys = jax.random.split(jax.random.fold_in(splits[12], 1), SEQ // ROWS)
    routes_turns = jax.random.permutation(jax.random.fold_in(splits[12], 3), SEQ // ROWS)
    routes = jax.vmap(lambda own, number: deal_out(jax.random.fold_in(splits[12], 2), own, number, ROWS, EXPERTS, TOPK, CAP, 2))(routes_keys, routes_turns).reshape((SEQ, TOPK))
    route_wt = jnp.clip(0.1 + 0.9 * jax.random.uniform(splits[13], (SEQ, TOPK), jnp.float32) ** level_of(splits[13], (SEQ, TOPK), ((0, 16),), -0.2, 0.2), 0.1, 1.0)
    exp_gate = centred(splits[14], (EXPERTS, D, FF), D ** -0.5, 0.125, ((0, 16), (2, 16)))
    exp_up = centred(splits[15], (EXPERTS, D, FF), D ** -0.5, 0.125, ((0, 16), (2, 16)))
    exp_down = centred(splits[16], (EXPERTS, FF, D), FF ** -0.5, 0.1875, ((0, 16), (1, 16)))
    return {"mix_in": mix_in, "gate_in": gate_in, "conv_w": conv_w, "conv_b": conv_b, "decay_param": decay_param, "recur_gate": recur_gate, "recur_bias": recur_bias, "input_gate": input_gate, "input_bias": input_bias, "residual": residual, "out_proj": out_proj, "norm_gain": norm_gain, "routes": routes, "route_wt": route_wt, "exp_gate": exp_gate, "exp_up": exp_up, "exp_down": exp_down}


EPSILON = 1e-06
HIGHEST_MODE = lax.Precision.HIGHEST

def norm_rows(values, gain):
    floats = values.astype(jnp.float32)
    return floats * lax.rsqrt(lax.optimization_barrier(jnp.mean(floats * floats, axis=-1, keepdims=True)) + EPSILON) * gain

def pair_join(earlier, later_pair):
    return (earlier[0] * later_pair[0], later_pair[0] * earlier[1] + later_pair[1])

def slot_table(route_rows, experts, capacity):
    row_count, top_count = route_rows.shape
    flattened = route_rows.reshape(row_count * top_count)
    matches = (flattened[:, None] == jnp.arange(experts, dtype=jnp.int32)[None, :]).astype(jnp.int32)
    earlier_hits = jnp.cumsum(matches, axis=0) - matches
    position = lax.optimization_barrier(jnp.sum(earlier_hits * matches, axis=1))
    return (flattened * capacity + position).reshape(row_count, top_count)

def coefficients(conv_out, recur_blocks, recur_bias, input_blocks, input_bias, decay_param):
    seq_len, channels = conv_out.shape
    heads, head_dim, _ = recur_blocks.shape
    blocked = conv_out.reshape(seq_len, heads, head_dim)
    recur_pre = jnp.einsum('lhi,hij->lhj', blocked, recur_blocks, precision=HIGHEST_MODE).reshape(seq_len, channels)
    input_pre = jnp.einsum('lhi,hij->lhj', blocked, input_blocks, precision=HIGHEST_MODE).reshape(seq_len, channels)
    recur_act = jax.nn.sigmoid(recur_pre + recur_bias)
    input_act = jax.nn.sigmoid(input_pre + input_bias)
    log_decay = -8.0 * recur_act * jax.nn.softplus(-decay_param)
    return (jnp.exp(log_decay), jnp.sqrt(-jnp.expm1(2.0 * log_decay)) * (input_act * conv_out))

def expert_apply(operands):
    tokens_in, gate_w, up_w, down_w = operands
    gate_act = jnp.dot(tokens_in, gate_w, preferred_element_type=jnp.float32)
    up_act = jnp.dot(tokens_in, up_w, preferred_element_type=jnp.float32)
    hidden = (jax.nn.silu(gate_act) * up_act).astype(jnp.bfloat16)
    return jnp.dot(hidden, down_w, preferred_element_type=jnp.float32).astype(jnp.bfloat16)

def reference(mix_in, gate_in, conv_w, conv_b, decay_param, recur_gate, recur_bias, input_gate, input_bias, residual, out_proj, norm_gain, routes, route_wt, exp_gate, exp_up, exp_down):
    seq_len = mix_in.shape[0]
    padded = jnp.pad(mix_in.astype(jnp.float32), ((2, 1), (0, 0)))
    conv_out = conv_b + padded[0:seq_len] * conv_w[0]
    for tap in range(1, conv_w.shape[0]):
        conv_out = conv_out + padded[tap:tap + seq_len] * conv_w[tap]
    state_sum = jnp.zeros_like(conv_out)
    for sense in range(2):
        decay, drive = coefficients(conv_out, recur_gate[sense], recur_bias[sense], input_gate[sense], input_bias[sense], decay_param[sense])
        if sense == 1:
            decay, drive = (jnp.flip(decay, 0), jnp.flip(drive, 0))
        _, states = lax.associative_scan(pair_join, (decay, drive), axis=0)
        if sense == 1:
            states = jnp.flip(states, 0)
        state_sum = state_sum + states
    mixed = (state_sum * jax.nn.gelu(gate_in.astype(jnp.float32))).astype(jnp.bfloat16)
    proj = jnp.dot(mixed, out_proj, preferred_element_type=jnp.float32).astype(jnp.bfloat16)
    proj = lax.optimization_barrier(proj)
    stream = (residual.astype(jnp.float32) + norm_rows(proj, norm_gain[0])).astype(jnp.bfloat16)
    stream = lax.optimization_barrier(stream)
    normed = norm_rows(stream, norm_gain[1]).astype(jnp.bfloat16)
    nblocks = seq_len // ROWS
    route_blocks = routes.reshape(nblocks, ROWS, TOPK)
    slots = jax.vmap(lambda block: slot_table(block, EXPERTS, CAP))(route_blocks)
    source_rows = jnp.repeat(jnp.arange(ROWS, dtype=jnp.int32), TOPK)

    def fill_table(slot_rows):
        empty = jnp.full((EXPERTS * CAP,), ROWS, jnp.int32)
        return empty.at[slot_rows.reshape(ROWS * TOPK)].set(source_rows)
    table = jax.vmap(fill_table)(slots)
    blocks_pad = jnp.concatenate([normed.reshape(nblocks, ROWS, D), jnp.zeros((nblocks, 1, D), jnp.bfloat16)], axis=1)
    dispatched = jnp.take_along_axis(blocks_pad, table[:, :, None], axis=1)
    by_expert = jnp.moveaxis(dispatched.reshape(nblocks, EXPERTS, CAP, D), 1, 0).reshape(EXPERTS, nblocks * CAP, D)
    results = lax.map(expert_apply, (by_expert, exp_gate, exp_up, exp_down)).reshape(EXPERTS, nblocks, CAP, D)
    slot_place = (slots % CAP).astype(jnp.int32)
    expert_ids = (slots // CAP).astype(jnp.int32)
    block_ids = jnp.arange(nblocks, dtype=jnp.int32)[:, None, None]
    picked = results[expert_ids, block_ids, slot_place]
    weights = route_wt.reshape(nblocks, ROWS, TOPK)[..., None]
    mixture = lax.optimization_barrier(jnp.sum(weights * picked.astype(jnp.float32), axis=2)).reshape(seq_len, D).astype(jnp.bfloat16)
    mixture = lax.optimization_barrier(mixture)
    return (stream.astype(jnp.float32) + norm_rows(mixture, norm_gain[2])).astype(jnp.bfloat16)
```

```python
import functools

import jax
import jax.numpy as jnp
from jax import lax
from jax.experimental import pallas as pl
from jax.experimental.pallas import tpu as pltpu
from jax.sharding import PartitionSpec as P

EPSILON = 1e-06
HIGHEST_MODE = lax.Precision.HIGHEST
MESH = pl.DeviceIdType.MESH
F32, BF16 = jnp.float32, jnp.bfloat16
SEGMENTS = 8
CHUNKS = 4


def hint(value, step):
    return pl.multiple_of(value, step)


def blocked_all(copy_ref, sem):
    pltpu.make_async_copy(copy_ref, copy_ref, sem).wait()


def root_mean(values):
    return lax.rsqrt(jnp.mean(values * values, axis=-1, keepdims=True) + EPSILON)


def ring_plan(nz):
    far, near = nz // 2, nz - 1 - nz // 2
    plans = []
    for direction in (0, 1):
        hops = lambda piece: far if (piece % 2 == direction) else near
        order = []
        groups = [(0, 1)] + [(2 + 2 * k, 3 + 2 * k) for k in range(CHUNKS // 2)]
        for group in groups:
            first = group if direction == 0 else group[::-1]
            for hop in range(1, far + 1):
                for piece in first:
                    if hop <= hops(piece):
                        order.append((piece, hop))
        plans.append(order)
    return plans


def kernel(
    n_sp,
    n_tp,
    mix_h,
    gate_h,
    conv_w,
    conv_b,
    decay,
    rg,
    rb,
    ig,
    ib,
    resid_h,
    oproj_h,
    gain,
    routes_h,
    wts_h,
    wg_h,
    wu_h,
    wd_h,
    out_ref,
    mixv,
    gatev,
    residv,
    oproj,
    routv,
    wtsv,
    halo,
    xpad,
    conv_s,
    wcat,
    ca0,
    cd0,
    ca1,
    cd1,
    stats,
    mixed,
    tokb,
    pbuf,
    stream_s,
    normed,
    outg,
    arr,
    wg,
    wu,
    wd,
    hid,
    outb,
    ret,
    wtab,
    load_sem,
    halo_send,
    halo_recv,
    stat_sem,
    tok_sem,
    disp_send,
    disp_recv,
    fwd_sem,
    hid_sem,
    pre_sem,
    ring_send,
    ring_recv,
    ret_send,
    ret_recv,
):
    nz = n_tp // 2
    sp, tp = lax.axis_index("sp"), lax.axis_index("tp")
    z, core = tp // 2, lax.rem(tp, 2)
    other = 1 - core
    sibling = 2 * z + other
    seq, chans = mix_h.shape
    rows, width = resid_h.shape
    half = width // 2
    hs = wg_h.shape[0]
    cap = outg.shape[0] // n_sp
    slots = n_sp * cap
    seg = seq // SEGMENTS
    cw = half // CHUNKS

    def load(src, dst, k):
        copy = pltpu.make_async_copy(src, dst, load_sem.at[k])
        copy.start()
        return copy

    own_rows = hint(tp * rows, rows)
    l_mix = load(mix_h, mixv, 0)
    l_gate = load(gate_h, gatev, 1)
    l_wg = load(wg_h, wg.at[z], 2)
    l_wu = load(wu_h, wu.at[z], 3)
    l_wd = load(
        wd_h.at[:, pl.ds(hint(core * half, half), half)],
        wd.at[core, pl.ds(hint(z * hs, hs), hs), :],
        4,
    )
    l_op = load(oproj_h, oproj, 5)
    l_res = load(resid_h, residv, 6)
    l_rt = load(routes_h, routv, 7)
    l_wt = load(wts_h, wtsv, 8)

    barrier = pltpu.get_barrier_semaphore()
    partners = []
    for i in range(1, n_sp):
        peer = lax.rem(sp + i, n_sp)
        partners += [(peer, tp), (peer, sibling)]
    for i in range(1, n_tp):
        partners.append((sp, lax.rem(tp + i, n_tp)))
    for peer in partners:
        pl.semaphore_signal(barrier, inc=1, device_id=peer, device_id_type=MESH)

    heads, hd = rg.shape[1], rg.shape[2]
    wcat[...] = jnp.zeros_like(wcat)
    for d in range(2):
        for which, ref in enumerate((rg, ig)):
            for h in range(heads):
                at = (2 * d + which) * chans + h * hd
                wcat[h * hd : (h + 1) * hd, at : at + hd] = ref[d, h]

    l_mix.wait()
    pl.semaphore_wait(barrier, len(partners))

    right = 2 * lax.rem(z + 1, nz) + core
    left = 2 * lax.rem(z + nz - 1, nz) + core

    def piece_ref(piece, shard):
        if piece == 0:
            return wg.at[shard]
        if piece == 1:
            return wu.at[shard]
        q = piece - 2
        return wd.at[:, pl.ds(hint(shard * hs, hs), hs), q * cw : (q + 1) * cw]

    def ring_copy(direction, piece, hop):
        back = (hop - 1) if direction == 0 else nz - (hop - 1)
        shard = lax.rem(z + nz - back, nz)
        dst = piece_ref(piece, shard)
        src = dst
        if hop == 1 and piece < 2:
            src = (wg_h, wu_h)[piece]
        return pltpu.make_async_remote_copy(
            src_ref=src,
            dst_ref=dst,
            send_sem=ring_send.at[direction, piece, hop - 1],
            recv_sem=ring_recv.at[direction, piece, hop - 1],
            device_id=(sp, right if direction == 0 else left),
            device_id_type=MESH,
        )

    def ring_arrived(direction, piece, hop):
        back = hop if direction == 0 else nz - hop
        shard = lax.rem(z + nz - back, nz)
        blocked_all(piece_ref(piece, shard), ring_recv.at[direction, piece, hop - 1])

    plans = ring_plan(nz)
    place = [0, 0]
    sent = []
    taken = set()

    def take(direction, piece, hop):
        if (direction, piece, hop) not in taken:
            taken.add((direction, piece, hop))
            ring_arrived(direction, piece, hop)

    def advance(count):
        for _ in range(count):
            for direction in (0, 1):
                if place[direction] < len(plans[direction]):
                    piece, hop = plans[direction][place[direction]]
                    place[direction] += 1
                    if hop > 1:
                        take(direction, piece, hop - 1)
                    ring_copy(direction, piece, hop).start()
                    sent.append((direction, piece, hop))

    def complete(piece):
        for direction in (0, 1):
            for p, hop in plans[direction]:
                if p == piece:
                    assert (direction, p, hop) in sent
                    take(direction, p, hop)

    nxt, prv = lax.rem(sp + 1, n_sp), lax.rem(sp + n_sp - 1, n_sp)
    hr = halo.shape[1]
    to_next = pltpu.make_async_remote_copy(
        src_ref=mixv.at[seq - hr : seq, :],
        dst_ref=halo.at[0],
        send_sem=halo_send.at[0],
        recv_sem=halo_recv.at[0],
        device_id=(nxt, tp),
        device_id_type=MESH,
    )
    to_prev = pltpu.make_async_remote_copy(
        src_ref=mixv.at[0:hr, :],
        dst_ref=halo.at[1],
        send_sem=halo_send.at[1],
        recv_sem=halo_recv.at[1],
        device_id=(prv, tp),
        device_id_type=MESH,
    )
    to_next.start()
    to_prev.start()

    pre = pltpu.make_async_remote_copy(
        src_ref=wd_h.at[:, pl.ds(hint(other * half, half), half)],
        dst_ref=wd.at[core, pl.ds(hint(z * hs, hs), hs), :],
        send_sem=pre_sem.at[0],
        recv_sem=pre_sem.at[1],
        device_id=(sp, sibling),
        device_id_type=MESH,
    )
    advance(2)
    pre.start()

    xpad[8 : 8 + seq, :] = mixv[...].astype(F32)
    to_next.wait()
    to_prev.wait()
    before = jnp.where(sp > 0, 1.0, 0.0).astype(F32)
    after = jnp.where(sp < n_sp - 1, 1.0, 0.0).astype(F32)
    xpad[0:8, :] = halo[0].astype(F32)[hr - 8 : hr] * before
    xpad[8 + seq : 16 + seq, :] = halo[1].astype(F32)[0:8] * after

    def strided(t):
        return xpad[pl.ds(t, SEGMENTS, stride=seg), :]

    taps = [jnp.broadcast_to(conv_w[j : j + 1, :], (SEGMENTS, chans)) for j in range(4)]
    bias = jnp.broadcast_to(conv_b[0:1, :], (SEGMENTS, chans))

    def conv_body(t, window):
        x0, x1, x2 = window
        x3 = strided(9 + t)
        conv_s[pl.ds(hint(t * SEGMENTS, SEGMENTS), SEGMENTS), :] = (
            bias + x0 * taps[0] + x1 * taps[1] + x2 * taps[2] + x3 * taps[3]
        )
        return x1, x2, x3

    lax.fori_loop(0, seg, conv_body, (strided(6), strided(7), strided(8)), unroll=8)

    rates = []
    for d in range(2):
        x = -decay[d : d + 1, :]
        rates.append(-8.0 * (jnp.maximum(x, 0.0) + jnp.log1p(jnp.exp(-jnp.abs(x)))))
    part = 128

    def coef_body(n, _):
        at = pl.ds(hint(n * part, part), part)
        c = conv_s[at, :]
        pre_act = jnp.dot(c, wcat[...], precision=HIGHEST_MODE, preferred_element_type=F32)
        for d, (a_ref, d_ref) in enumerate(((ca0, cd0), (ca1, cd1))):
            r = jax.nn.sigmoid(pre_act[:, 2 * d * chans : (2 * d + 1) * chans] + rb[d : d + 1, :])
            i = jax.nn.sigmoid(
                pre_act[:, (2 * d + 1) * chans : (2 * d + 2) * chans] + ib[d : d + 1, :]
            )
            la = r * rates[d]
            a = jnp.exp(la)
            x = 2.0 * la
            series = 1.0 + x * (1.0 / 6.0)
            for k in (5.0, 4.0, 3.0, 2.0):
                series = 1.0 + x * (1.0 / k) * series
            gap = jnp.where(x > -0.3, -x * series, 1.0 - a * a)
            a_ref[at, :] = a
            d_ref[at, :] = jnp.sqrt(gap) * (i * c)
        return 0

    lax.fori_loop(0, seq // part, coef_body, 0)

    zero = jnp.zeros((SEGMENTS, chans), F32)
    one = jnp.ones((SEGMENTS, chans), F32)

    def scan_body(t, carry):
        f, p, g, q = carry
        fat = pl.ds(hint(t * SEGMENTS, SEGMENTS), SEGMENTS)
        bat = pl.ds(hint((seg - 1 - t) * SEGMENTS, SEGMENTS), SEGMENTS)
        a, b = ca0[fat, :], ca1[bat, :]
        f = a * f + cd0[fat, :]
        p = a * p
        g = b * g + cd1[bat, :]
        q = b * q
        cd0[fat, :] = f
        ca0[fat, :] = p
        cd1[bat, :] = g
        ca1[bat, :] = q
        return f, p, g, q

    f_end, p_end, g_end, q_end = lax.fori_loop(0, seg, scan_body, (zero, one, zero, one), unroll=8)

    row = lambda v, k: v[k : k + 1, :]
    f_scale, f_shift = [row(one, 0)], [row(zero, 0)]
    for k in range(SEGMENTS):
        f_scale.append(row(p_end, k) * f_scale[-1])
        f_shift.append(row(p_end, k) * f_shift[-1] + row(f_end, k))
    b_scale, b_shift = [row(one, 0)], [row(zero, 0)]
    for k in range(SEGMENTS - 1, -1, -1):
        b_scale.append(row(q_end, k) * b_scale[-1])
        b_shift.append(row(q_end, k) * b_shift[-1] + row(g_end, k))
    for k, v in enumerate((f_scale[-1], f_shift[-1], b_scale[-1], b_shift[-1])):
        stats[sp, k : k + 1, :] = v
    for i in range(1, n_sp):
        pltpu.make_async_remote_copy(
            src_ref=stats.at[sp],
            dst_ref=stats.at[sp],
            send_sem=stat_sem.at[0],
            recv_sem=stat_sem.at[1],
            device_id=(lax.rem(sp + i, n_sp), tp),
            device_id_type=MESH,
        ).start()

    l_gate.wait()

    def gelu_body(n, _):
        at = pl.ds(hint(n * 64, 64), 64)
        xpad[at, :] = jax.nn.gelu(gatev[at, :].astype(F32))
        return 0

    lax.fori_loop(0, seq // 64, gelu_body, 0)
    blocked_all(stats.at[0 : n_sp - 1], stat_sem.at[1])

    f_in = jnp.zeros((1, chans), F32)
    b_in = jnp.zeros((1, chans), F32)
    for j in range(n_sp):
        f_in = jnp.where(j < sp, stats[j, 0:1, :] * f_in + stats[j, 1:2, :], f_in)
        k = n_sp - 1 - j
        b_in = jnp.where(k > sp, stats[k, 2:3, :] * b_in + stats[k, 3:4, :], b_in)
    f_enter = jnp.concatenate(
        [f_scale[k] * f_in + f_shift[k] for k in range(SEGMENTS)], axis=0
    )
    b_enter = jnp.concatenate(
        [b_scale[SEGMENTS - 1 - k] * b_in + b_shift[SEGMENTS - 1 - k] for k in range(SEGMENTS)],
        axis=0,
    )

    def join_body(t, _):
        at = pl.ds(hint(t * SEGMENTS, SEGMENTS), SEGMENTS)
        back = pl.ds(t, SEGMENTS, stride=seg)
        state = (cd0[at, :] + ca0[at, :] * f_enter) + (cd1[at, :] + ca1[at, :] * b_enter)
        conv_s[back, :] = state
        return 0

    lax.fori_loop(0, seg, join_body, 0, unroll=8)

    def mix_body(n, _):
        at = pl.ds(hint(n * rows, rows), rows)
        mixed[at, :] = (conv_s[at, :] * xpad[at, :]).astype(BF16)
        return 0

    lax.fori_loop(0, seq // rows, mix_body, 0)

    own_cols = pl.ds(hint(tp * chans, chans), chans)
    for i in range(1, n_tp):
        peer = lax.rem(tp + i, n_tp)
        pltpu.make_async_remote_copy(
            src_ref=mixed.at[pl.ds(hint(peer * rows, rows), rows), :],
            dst_ref=tokb.at[:, own_cols],
            send_sem=tok_sem.at[0],
            recv_sem=tok_sem.at[1],
            device_id=(sp, peer),
            device_id_type=MESH,
        ).start()
    tokb[:, own_cols] = mixed[pl.ds(own_rows, rows), :]
    advance(1)

    l_rt.wait()
    l_wt.wait()
    lane = lax.broadcasted_iota(jnp.int32, (n_sp, rows), 0)
    own_routes = routv[tp]
    own_wts = wtsv[tp]
    e0 = jnp.broadcast_to(own_routes[0:1, :], (n_sp, rows))
    e1 = jnp.broadcast_to(own_routes[1:2, :], (n_sp, rows))
    h0 = jnp.where(e0 == lane, 1.0, 0.0)
    h1 = jnp.where(e1 == lane, 1.0, 0.0)
    earlier = jnp.where(
        lax.broadcasted_iota(jnp.int32, (rows, rows), 0)
        < lax.broadcasted_iota(jnp.int32, (rows, rows), 1),
        1.0,
        0.0,
    )
    counts = jnp.dot(
        (h0 + h1).astype(BF16), earlier.astype(BF16), preferred_element_type=F32
    )
    slot0 = jnp.sum(counts * h0, axis=0, keepdims=True).astype(jnp.int32) + own_routes[
        0:1, :
    ] * cap
    slot1 = jnp.sum(counts * h1, axis=0, keepdims=True).astype(jnp.int32) + own_routes[
        1:2, :
    ] * cap
    slot_id = lax.broadcasted_iota(jnp.int32, (slots, rows), 0)
    hit0, hit1 = slot_id == slot0, slot_id == slot1
    sel = jnp.where(hit0 | hit1, 1.0, 0.0).astype(BF16)
    weights = jnp.where(hit0, own_wts[0:1, :], 0.0) + jnp.where(hit1, own_wts[1:2, :], 0.0)
    eye = jnp.where(
        lax.broadcasted_iota(jnp.int32, (rows, rows), 0)
        == lax.broadcasted_iota(jnp.int32, (rows, rows), 1),
        1.0,
        0.0,
    )
    table = lax.dot_general(
        eye,
        weights,
        (((1,), (1,)), ((), ())),
        precision=HIGHEST_MODE,
        preferred_element_type=F32,
    )
    high = table.astype(BF16)
    wtab[0] = high
    wtab[1] = (table - high.astype(F32)).astype(BF16)

    l_op.wait()
    l_res.wait()
    blocked_all(tokb.at[:, 0 : (n_tp - 1) * chans], tok_sem.at[1])
    advance(1)
    pw = min(512, width)

    def proj_body(n, _):
        at = pl.ds(hint(n * pw, pw), pw)
        pbuf[:, at] = (
            jnp.dot(tokb[...], oproj[:, at], preferred_element_type=F32).astype(BF16).astype(F32)
        )
        return 0

    lax.fori_loop(0, width // pw, proj_body, 0)

    def norm_body(n, _):
        at = pl.ds(hint(n * 16, 16), 16)
        v = pbuf[at, :]
        s = (residv[at, :].astype(F32) + v * root_mean(v) * gain[0:1, :]).astype(BF16).astype(F32)
        stream_s[at, :] = s
        normed[at, :] = (s * root_mean(s) * gain[1:2, :]).astype(BF16)
        return 0

    lax.fori_loop(0, rows // 16, norm_body, 0)

    gw = min(256, width)

    def dispatch_body(n, _):
        at = pl.ds(hint(n * gw, gw), gw)
        outg[:, at] = jnp.dot(sel, normed[:, at], preferred_element_type=F32).astype(BF16)
        return 0

    lax.fori_loop(0, width // gw, dispatch_body, 0)
    own_slots = pl.ds(hint(sp * cap, cap), cap)
    for i in range(1, n_sp):
        peer = lax.rem(sp + i, n_sp)
        pltpu.make_async_remote_copy(
            src_ref=outg.at[pl.ds(hint(peer * cap, cap), cap), :],
            dst_ref=arr.at[core, own_slots, :],
            send_sem=disp_send.at[0],
            recv_sem=disp_recv.at[i - 1],
            device_id=(peer, tp),
            device_id_type=MESH,
        ).start()

    def forward(src_ref, at):
        pltpu.make_async_remote_copy(
            src_ref=src_ref,
            dst_ref=arr.at[core, at, :],
            send_sem=fwd_sem.at[0],
            recv_sem=fwd_sem.at[1],
            device_id=(sp, sibling),
            device_id_type=MESH,
        ).start()

    forward(outg.at[own_slots, :], own_slots)
    arr[core, own_slots, :] = outg[own_slots, :]
    advance(1)
    for i in range(1, n_sp):
        src = lax.rem(sp + n_sp - i, n_sp)
        at = pl.ds(hint(src * cap, cap), cap)
        blocked_all(arr.at[core, at, :], disp_recv.at[i - 1])
        forward(arr.at[core, at, :], at)
        if i == n_sp // 2:
            advance(1)

    while not all(
        any(ev == (p, h) for ev in plans[d][: place[d]])
        for d in (0, 1)
        for p, h in plans[d]
        if p < 2
    ):
        advance(1)
    l_wg.wait()
    l_wu.wait()
    l_wd.wait()
    pre.wait()
    advance(2)
    blocked_all(arr.at[other], fwd_sem.at[1])
    complete(0)
    complete(1)
    advance(2)
    hidden_all = nz * hs
    hw = min(256, hidden_all)
    hm = min(256, slots)
    zh = hw // hs
    per = slots // hm

    def gate_body(n, _):
        c, m = n // per, lax.rem(n, per)
        at = pl.ds(hint(m * hm, hm), hm)
        x = arr[c, at, :]
        for k in range(hidden_all // hw):
            dims = (((1,), (1,)), ((), ()))
            g = lax.dot_general(
                x,
                wg[k * zh : (k + 1) * zh].reshape(hw, width),
                dims,
                preferred_element_type=F32,
            )
            u = lax.dot_general(
                x,
                wu[k * zh : (k + 1) * zh].reshape(hw, width),
                dims,
                preferred_element_type=F32,
            )
            hid[core, pl.ds(hint(n * hm, hm), hm), k * hw : (k + 1) * hw] = (
                g * jax.nn.sigmoid(g) * u
            ).astype(BF16)
        return 0

    lax.fori_loop(0, 2 * per, gate_body, 0)
    swap = pltpu.make_async_remote_copy(
        src_ref=hid.at[core],
        dst_ref=hid.at[core],
        send_sem=hid_sem.at[0],
        recv_sem=hid_sem.at[1],
        device_id=(sp, sibling),
        device_id_type=MESH,
    )
    swap.start()
    advance(1)
    swap.wait_recv()

    for q in range(CHUNKS):
        while not all(
            any(ev == (p, h) for ev in plans[d][: place[d]])
            for d in (0, 1)
            for p, h in plans[d]
            if p == 2 + q
        ):
            advance(1)
        advance(1)
        complete(2 + q)

        def down_body(n, _):
            at = pl.ds(hint(n * hm, hm), hm)
            o = jnp.dot(
                hid[0, at, :], wd[0, :, q * cw : (q + 1) * cw], preferred_element_type=F32
            ) + jnp.dot(hid[1, at, :], wd[1, :, q * cw : (q + 1) * cw], preferred_element_type=F32)
            outb[q, at, :] = o.astype(BF16)
            return 0

        lax.fori_loop(0, 2 * per, down_body, 0)
        for i in range(n_sp):
            peer = lax.rem(sp + i, n_sp)
            for mine in (1, 0):
                if i == 0 and mine:
                    continue
                c = core if mine else other
                pltpu.make_async_remote_copy(
                    src_ref=outb.at[q, pl.ds(hint(c * slots + peer * cap, cap), cap), :],
                    dst_ref=ret.at[core, q, own_slots, :],
                    send_sem=ret_send.at[q, mine],
                    recv_sem=ret_recv.at[q, mine],
                    device_id=(peer, tp if mine else sibling),
                    device_id_type=MESH,
                ).start()
        ret[core, q, own_slots, :] = outb[
            q, pl.ds(hint(core * slots + sp * cap, cap), cap), :
        ]

    for q in range(CHUNKS):
        blocked_all(ret.at[core, q, 0 : slots - cap, :], ret_recv.at[q, 1])
        blocked_all(ret.at[other, q], ret_recv.at[q, 0])
        for c in range(2):
            v = ret[c, q]
            o = jnp.dot(wtab[0], v, preferred_element_type=F32) + jnp.dot(
                wtab[1], v, preferred_element_type=F32
            )
            pbuf[:, c * half + q * cw : c * half + (q + 1) * cw] = o.astype(BF16).astype(F32)

    def final_body(n, _):
        at = pl.ds(hint(n * 16, 16), 16)
        v = pbuf[at, :]
        out_ref[at, :] = (stream_s[at, :] + v * root_mean(v) * gain[2:3, :]).astype(BF16)
        return 0

    lax.fori_loop(0, rows // 16, final_body, 0)

    blocked_all(stats.at[0 : n_sp - 1], stat_sem.at[0])
    blocked_all(tokb.at[:, 0 : (n_tp - 1) * chans], tok_sem.at[0])
    blocked_all(outg.at[0 : slots - cap, :], disp_send.at[0])
    blocked_all(outg, fwd_sem.at[0])
    swap.wait_send()
    for q in range(CHUNKS):
        blocked_all(ret.at[core, q, 0 : slots - cap, :], ret_send.at[q, 1])
        blocked_all(ret.at[other, q], ret_send.at[q, 0])
    for event in sent:
        ring_copy(*event).wait_send()


def on_device(
    mix_in,
    gate_in,
    conv_w,
    conv_b,
    decay_param,
    recur_gate,
    recur_bias,
    input_gate,
    input_bias,
    residual,
    out_proj,
    norm_gain,
    routes,
    route_wt,
    exp_gate,
    exp_up,
    exp_down,
):
    n_sp, n_tp = lax.axis_size("sp"), lax.axis_size("tp")
    nz = n_tp // 2
    seq, chans = mix_in.shape
    rows, width = residual.shape
    top = routes.shape[1]
    experts = n_sp * exp_gate.shape[0]
    cap = 2 * rows * top // experts
    slots = experts * cap
    hs = exp_gate.shape[2]
    half = width // 2
    far = nz // 2
    pieces = 2 + CHUNKS

    def tables(array):
        return array.T.reshape(top, n_tp, rows).transpose(1, 0, 2)

    anywhere = pl.BlockSpec(memory_space=pl.ANY)
    onchip = pl.BlockSpec(memory_space=pltpu.VMEM)
    dma = pltpu.SemaphoreType.DMA
    scratch = [
        pltpu.VMEM((seq, chans), BF16),
        pltpu.VMEM((seq, chans), BF16),
        pltpu.VMEM((rows, width), BF16),
        pltpu.VMEM(out_proj.shape, BF16),
        pltpu.VMEM((n_tp, top, rows), jnp.int32),
        pltpu.VMEM((n_tp, top, rows), F32),
        pltpu.VMEM((2, 16, chans), BF16),
        pltpu.VMEM((seq + 16, chans), F32),
        pltpu.VMEM((seq, chans), F32),
        pltpu.VMEM((chans, 4 * chans), F32),
        pltpu.VMEM((seq, chans), F32),
        pltpu.VMEM((seq, chans), F32),
        pltpu.VMEM((seq, chans), F32),
        pltpu.VMEM((seq, chans), F32),
        pltpu.VMEM((n_sp, 8, chans), F32),
        pltpu.VMEM((seq, chans), BF16),
        pltpu.VMEM((rows, n_tp * chans), BF16),
        pltpu.VMEM((rows, width), F32),
        pltpu.VMEM((rows, width), F32),
        pltpu.VMEM((rows, width), BF16),
        pltpu.VMEM((slots, width), BF16),
        pltpu.VMEM((2, slots, width), BF16),
        pltpu.VMEM((nz, hs, width), BF16),
        pltpu.VMEM((nz, hs, width), BF16),
        pltpu.VMEM((2, nz * hs, half), BF16),
        pltpu.VMEM((2, 2 * slots, nz * hs), BF16),
        pltpu.VMEM((CHUNKS, 2 * slots, half // CHUNKS), BF16),
        pltpu.VMEM((2, CHUNKS, slots, half // CHUNKS), BF16),
        pltpu.VMEM((2, rows, slots), BF16),
        dma((9,)),
        dma((2,)),
        dma((2,)),
        dma((2,)),
        dma((2,)),
        dma((1,)),
        dma((n_sp - 1,)),
        dma((2,)),
        dma((2,)),
        dma((2,)),
        dma((2, pieces, far)),
        dma((2, pieces, far)),
        dma((CHUNKS, 2)),
        dma((CHUNKS, 2)),
    ]
    where = [
        anywhere,
        anywhere,
        onchip,
        onchip,
        onchip,
        onchip,
        onchip,
        onchip,
        onchip,
        anywhere,
        anywhere,
        onchip,
        anywhere,
        anywhere,
        anywhere,
        anywhere,
        anywhere,
    ]
    return pl.pallas_call(
        functools.partial(kernel, n_sp, n_tp),
        out_shape=jax.ShapeDtypeStruct((rows, width), BF16),
        in_specs=where,
        out_specs=onchip,
        scratch_shapes=scratch,
        compiler_params=pltpu.CompilerParams(
            collective_id=0, has_side_effects=True, vmem_limit_bytes=60 * 1024 * 1024
        ),
    )(
        mix_in,
        gate_in,
        conv_w,
        conv_b.reshape(1, chans),
        decay_param,
        recur_gate,
        recur_bias,
        input_gate,
        input_bias,
        residual,
        out_proj,
        norm_gain,
        tables(routes),
        tables(route_wt),
        exp_gate[0].T,
        exp_up[0].T,
        exp_down[0],
    )


def solution(mesh):
    return jax.shard_map(
        on_device,
        mesh=mesh,
        in_specs=(
            P("sp", "tp"),
            P("sp", "tp"),
            P(None, "tp"),
            P("tp"),
            P(None, "tp"),
            P(None, "tp", None, None),
            P(None, "tp"),
            P(None, "tp", None, None),
            P(None, "tp"),
            P(("sp", "tp"), None),
            P(),
            P(),
            P("sp", None),
            P("sp", None),
            P("sp", None, "tp"),
            P("sp", None, "tp"),
            P("sp", "tp", None),
        ),
        out_specs=P(("sp", "tp"), None),
        check_vma=False,
    )
```

```python
import functools

import jax
import jax.numpy as jnp
from jax import lax
from jax.experimental import pallas as pl
from jax.experimental.pallas import tpu as pltpu
from jax.sharding import PartitionSpec as P

EPSILON = 1e-06
HIGHEST_MODE = lax.Precision.HIGHEST
MESH = pl.DeviceIdType.MESH
F32, BF16 = jnp.float32, jnp.bfloat16
SEGMENTS = 8
WIDTHS = (128, 128, 128, 128, 256, 256)
CHUNKS = len(WIDTHS)
NEVER = 1 << 20
PLAN = (
    ((0, 0, 1), (0, 1, 1), (1, 1, 1), (1, 0, 1),),
    (),
    ((0, 4, 1), (0, 5, 1), (0, 2, 1), (0, 3, 1), (1, 4, 1), (1, 5, 1), (1, 2, 1), (1, 3, 1),),
    (),
    (),
    (),
    ((0, 0, 2), (1, 1, 2),),
    (),
    ((0, 1, 2), (1, 0, 2), (0, 0, 3), (1, 2, 2), (1, 1, 3),),
    (),
    (),
    (),
    (),
    (),
    ((0, 2, 2), (0, 3, 2), (0, 4, 2), (0, 5, 2), (0, 6, 1), (1, 3, 2), (1, 4, 2), (1, 5, 2), (1, 6, 1), (0, 1, 3), (1, 7, 1), (1, 2, 3),),
    (),
    ((1, 0, 3),),
    (),
    (),
    (),
    (),
    ((0, 2, 3),),
    ((0, 3, 3), (1, 3, 3),),
    (),
    (),
    ((0, 0, 4), (1, 1, 4),),
    (),
    (),
    (),
    (),
    ((0, 6, 2), (0, 7, 1), (0, 4, 3), (1, 6, 2), (1, 7, 2),),
    (),
    ((0, 2, 4), (1, 3, 4),),
    ((0, 6, 3), (1, 4, 3),),
    ((1, 5, 3),),
    ((0, 4, 4), (1, 6, 3),),
    ((0, 7, 2),),
    (),
    (),
    (),
    ((1, 7, 3),),
    (),
    (),
    (),
    ((0, 5, 3),),
    (),
    (),
    (),
    ((0, 6, 4), (1, 5, 4),),
    (),
    (),
    (),
    (),
    ((0, 7, 3), (1, 7, 4),),
    (),
    (),
    (),
    (),
    (),
    (),
    (),
    (),
    (),
    (),
    (),
    (),
)
STARTS = tuple(sum(WIDTHS[:k]) for k in range(CHUNKS))


def hint(value, step):
    return pl.multiple_of(value, step)


def blocked_all(copy_ref, sem):
    pltpu.make_async_copy(copy_ref, copy_ref, sem).wait()


def root_mean(values):
    return lax.rsqrt(jnp.mean(values * values, axis=-1, keepdims=True) + EPSILON)


def places(nz):
    order = [0]
    for step in range(1, nz // 2 + 1):
        order += [step, nz - step] if step < nz - step else [step]
    return {distance: place for place, distance in enumerate(order)}


def kernel(
    n_sp,
    n_tp,
    mix_h,
    gate_h,
    conv_w,
    conv_b,
    decay,
    rg,
    rb,
    ig,
    ib,
    resid_h,
    oproj_h,
    gain,
    routes_h,
    wts_h,
    wg_h,
    wu_h,
    wd_h,
    out_ref,
    mixv,
    gatev,
    residv,
    oproj,
    routv,
    wtsv,
    halo,
    xpad,
    conv_s,
    wcat,
    ca0,
    cd0,
    ca1,
    cd1,
    stats,
    mixed,
    tokb,
    pbuf,
    stream_s,
    normed,
    outg,
    arr,
    wg,
    wu,
    wd,
    hid,
    outb,
    ret,
    wtab,
    load_sem,
    halo_send,
    halo_recv,
    stat_sem,
    tok_sem,
    disp_send,
    disp_recv,
    fwd_sem,
    hid_send,
    hid_recv,
    pre_sem,
    ring_send,
    ring_recv,
    ret_send,
    ret_recv,
):
    nz = n_tp // 2
    sp, tp = lax.axis_index("sp"), lax.axis_index("tp")
    z, core = tp // 2, lax.rem(tp, 2)
    other = 1 - core
    sibling = 2 * z + other
    seq, chans = mix_h.shape
    rows, width = resid_h.shape
    half = width // 2
    hs = wg_h.shape[0]
    cap = outg.shape[0] // n_sp
    slots = n_sp * cap
    seg = seq // SEGMENTS

    loads = {}
    drains = []

    def load(src, dst, k):
        copy = pltpu.make_async_copy(src, dst, load_sem.at[k])
        copy.start()
        loads[k] = copy
        return k

    def need(k):
        if k in loads:
            loads.pop(k).wait()

    own_rows = hint(tp * rows, rows)
    l_mix = load(mix_h, mixv, 0)
    l_gate = load(gate_h, gatev, 1)
    l_wg = load(wg_h, wg.at[0], 2)
    l_wu = load(wu_h, wu.at[0], 3)
    l_wd = load(
        wd_h.at[:, pl.ds(hint(core * half, half), half)],
        wd.at[core, 0:hs, :],
        4,
    )
    l_op = load(oproj_h, oproj, 5)
    l_res = load(resid_h, residv, 6)
    pair = pl.ds(hint(z * 2 * rows, 2 * rows), 2 * rows)
    l_rt = load(routes_h.at[:, pair], routv, 7)
    l_wt = load(wts_h.at[:, pair], wtsv, 8)

    barrier = pltpu.get_barrier_semaphore()
    partners = []
    for i in range(1, n_sp):
        peer = lax.rem(sp + i, n_sp)
        partners += [(peer, tp), (peer, sibling)]
    for i in range(1, n_tp):
        partners.append((sp, lax.rem(tp + i, n_tp)))
    for peer in partners:
        pl.semaphore_signal(barrier, inc=1, device_id=peer, device_id_type=MESH)

    heads, hd = rg.shape[1], rg.shape[2]
    wcat[...] = jnp.zeros_like(wcat)
    for d in range(2):
        for which, ref in enumerate((rg, ig)):
            for h in range(heads):
                at = (2 * d + which) * chans + h * hd
                wcat[h * hd : (h + 1) * hd, at : at + hd] = ref[d, h]

    need(l_mix)
    pl.semaphore_wait(barrier, len(partners))

    right = 2 * lax.rem(z + 1, nz) + core
    left = 2 * lax.rem(z + nz - 1, nz) + core

    far, near = nz // 2, nz - 1 - nz // 2
    place = places(nz)

    def hops(direction, piece):
        return far if piece % 2 == direction else near

    def piece_ref(direction, piece, hop):
        at = place[hop if direction == 1 or hop == 0 else nz - hop]
        if piece < 2:
            return (wg, wu)[piece].at[at]
        q = piece - 2
        return wd.at[:, at * hs : (at + 1) * hs, STARTS[q] : STARTS[q] + WIDTHS[q]]

    def ring_copy(direction, piece, hop):
        src = piece_ref(direction, piece, hop - 1)
        if hop == 1 and piece < 2:
            src = (wg_h, wu_h)[piece]
        return pltpu.make_async_remote_copy(
            src_ref=src,
            dst_ref=piece_ref(direction, piece, hop),
            send_sem=ring_send.at[direction, piece, hop - 1],
            recv_sem=ring_recv.at[direction, piece, hop - 1],
            device_id=(sp, right if direction == 0 else left),
            device_id_type=MESH,
        )

    sent = []
    taken = set()
    stage = [0]

    def take(direction, piece, hop):
        if (direction, piece, hop) not in taken:
            taken.add((direction, piece, hop))
            blocked_all(
                piece_ref(direction, piece, hop), ring_recv.at[direction, piece, hop - 1]
            )

    def poll():
        for direction, piece, hop in PLAN[stage[0]]:
            if hop > 1:
                take(direction, piece, hop - 1)
            elif piece >= 2 and "pre" not in taken:
                taken.add("pre")
                need(l_wd)
                pre.wait()
            ring_copy(direction, piece, hop).start()
            sent.append((direction, piece, hop))
        stage[0] += 1

    def complete(piece, end=NEVER):
        for direction in (0, 1):
            for hop in range(1, hops(direction, piece) + 1):
                if place[hop if direction == 1 else nz - hop] < end:
                    assert (direction, piece, hop) in sent
                    take(direction, piece, hop)

    def finish():
        for drain in drains:
            drain()
        for event in sent:
            ring_copy(*event).wait_send()

    nxt, prv = lax.rem(sp + 1, n_sp), lax.rem(sp + n_sp - 1, n_sp)
    hr = halo.shape[1]
    to_next = pltpu.make_async_remote_copy(
        src_ref=mixv.at[seq - hr : seq, :],
        dst_ref=halo.at[0],
        send_sem=halo_send.at[0],
        recv_sem=halo_recv.at[0],
        device_id=(nxt, tp),
        device_id_type=MESH,
    )
    to_prev = pltpu.make_async_remote_copy(
        src_ref=mixv.at[0:hr, :],
        dst_ref=halo.at[1],
        send_sem=halo_send.at[1],
        recv_sem=halo_recv.at[1],
        device_id=(prv, tp),
        device_id_type=MESH,
    )
    to_next.start()
    to_prev.start()

    pre = pltpu.make_async_remote_copy(
        src_ref=wd_h.at[:, pl.ds(hint(other * half, half), half)],
        dst_ref=wd.at[core, 0:hs, :],
        send_sem=pre_sem.at[0],
        recv_sem=pre_sem.at[1],
        device_id=(sp, sibling),
        device_id_type=MESH,
    )
    poll()
    pre.start()

    xpad[0:8, :] = jnp.zeros((8, chans), F32)
    xpad[8 : 8 + seq, :] = mixv[...].astype(F32)
    xpad[8 + seq : 16 + seq, :] = jnp.zeros((8, chans), F32)

    def strided(t):
        return xpad[pl.ds(t, SEGMENTS, stride=seg), :]

    taps = [jnp.broadcast_to(conv_w[j : j + 1, :], (SEGMENTS, chans)) for j in range(4)]
    bias = jnp.broadcast_to(conv_b[0:1, :], (SEGMENTS, chans))

    def weigh(x0, x1, x2, x3):
        return bias + x0 * taps[0] + x1 * taps[1] + x2 * taps[2] + x3 * taps[3]

    def conv_body(t, window):
        x0, x1, x2 = window
        x3 = strided(9 + t)
        conv_s[pl.ds(hint(t * SEGMENTS, SEGMENTS), SEGMENTS), :] = weigh(x0, x1, x2, x3)
        return x1, x2, x3

    lax.fori_loop(0, seg, conv_body, (strided(6), strided(7), strided(8)), unroll=8)

    rates = []
    for d in range(2):
        x = -decay[d : d + 1, :]
        rates.append(-8.0 * (jnp.maximum(x, 0.0) + jnp.log1p(jnp.exp(-jnp.abs(x)))))
    part = 128

    def coefficients(c):
        pre_act = jnp.dot(c, wcat[...], precision=HIGHEST_MODE, preferred_element_type=F32)
        found = []
        for d in range(2):
            r = jax.nn.sigmoid(pre_act[:, 2 * d * chans : (2 * d + 1) * chans] + rb[d : d + 1, :])
            i = jax.nn.sigmoid(
                pre_act[:, (2 * d + 1) * chans : (2 * d + 2) * chans] + ib[d : d + 1, :]
            )
            la = r * rates[d]
            a = jnp.exp(la)
            x = 2.0 * la
            series = 1.0 + x * (1.0 / 6.0)
            for k in (5.0, 4.0, 3.0, 2.0):
                series = 1.0 + x * (1.0 / k) * series
            gap = jnp.where(x > -0.3, -x * series, 1.0 - a * a)
            found += [a, jnp.sqrt(gap) * (i * c)]
        return found

    kept = (ca0, cd0, ca1, cd1)

    def coef_body(n, _):
        at = pl.ds(hint(n * part, part), part)
        for ref, value in zip(kept, coefficients(conv_s[at, :])):
            ref[at, :] = value
        return 0

    lax.fori_loop(0, seq // part // 2, coef_body, 0)
    poll()
    lax.fori_loop(seq // part // 2, seq // part, coef_body, 0)

    poll()
    to_next.wait()
    to_prev.wait()
    before = jnp.where(sp > 0, 1.0, 0.0).astype(F32)
    after = jnp.where(sp < n_sp - 1, 1.0, 0.0).astype(F32)
    xpad[0:8, :] = halo[0].astype(F32)[hr - 8 : hr] * before
    xpad[8 + seq : 16 + seq, :] = halo[1].astype(F32)[0:8] * after
    ends = jnp.concatenate(
        [weigh(*(strided(6 + t + j) for j in range(4))) for t in (0, 1, seg - 1)], axis=0
    )
    for ref, value in zip(kept, coefficients(ends)):
        ref[0 : 2 * SEGMENTS, :] = value[0 : 2 * SEGMENTS]
        ref[seq - SEGMENTS : seq, :] = value[2 * SEGMENTS :]

    zero = jnp.zeros((SEGMENTS, chans), F32)
    one = jnp.ones((SEGMENTS, chans), F32)

    def scan_body(t, carry):
        f, p, g, q = carry
        fat = pl.ds(hint(t * SEGMENTS, SEGMENTS), SEGMENTS)
        bat = pl.ds(hint((seg - 1 - t) * SEGMENTS, SEGMENTS), SEGMENTS)
        a, b = ca0[fat, :], ca1[bat, :]
        f = a * f + cd0[fat, :]
        p = a * p
        g = b * g + cd1[bat, :]
        q = b * q
        cd0[fat, :] = f
        ca0[fat, :] = p
        cd1[bat, :] = g
        ca1[bat, :] = q
        return f, p, g, q

    f_end, p_end, g_end, q_end = lax.fori_loop(0, seg, scan_body, (zero, one, zero, one), unroll=8)

    poll()

    row = lambda v, k: v[k : k + 1, :]
    f_scale, f_shift = [row(one, 0)], [row(zero, 0)]
    for k in range(SEGMENTS):
        f_scale.append(row(p_end, k) * f_scale[-1])
        f_shift.append(row(p_end, k) * f_shift[-1] + row(f_end, k))
    b_scale, b_shift = [row(one, 0)], [row(zero, 0)]
    for k in range(SEGMENTS - 1, -1, -1):
        b_scale.append(row(q_end, k) * b_scale[-1])
        b_shift.append(row(q_end, k) * b_shift[-1] + row(g_end, k))
    for k, v in enumerate((f_scale[-1], f_shift[-1], b_scale[-1], b_shift[-1])):
        stats[sp, k : k + 1, :] = v
    for i in range(1, n_sp):
        pltpu.make_async_remote_copy(
            src_ref=stats.at[sp],
            dst_ref=stats.at[sp],
            send_sem=stat_sem.at[0],
            recv_sem=stat_sem.at[1],
            device_id=(lax.rem(sp + i, n_sp), tp),
            device_id_type=MESH,
        ).start()
    drains.append(lambda: blocked_all(stats.at[0 : n_sp - 1], stat_sem.at[0]))
    poll()

    need(l_gate)

    def gelu_body(n, _):
        at = pl.ds(hint(n * 64, 64), 64)
        xpad[at, :] = jax.nn.gelu(gatev[at, :].astype(F32))
        return 0

    lax.fori_loop(0, seq // 64, gelu_body, 0)
    poll()
    blocked_all(stats.at[0 : n_sp - 1], stat_sem.at[1])

    f_in = jnp.zeros((1, chans), F32)
    b_in = jnp.zeros((1, chans), F32)
    for j in range(n_sp):
        f_in = jnp.where(j < sp, stats[j, 0:1, :] * f_in + stats[j, 1:2, :], f_in)
        k = n_sp - 1 - j
        b_in = jnp.where(k > sp, stats[k, 2:3, :] * b_in + stats[k, 3:4, :], b_in)
    f_enter = jnp.concatenate(
        [f_scale[k] * f_in + f_shift[k] for k in range(SEGMENTS)], axis=0
    )
    b_enter = jnp.concatenate(
        [b_scale[SEGMENTS - 1 - k] * b_in + b_shift[SEGMENTS - 1 - k] for k in range(SEGMENTS)],
        axis=0,
    )

    def join_body(t, _):
        at = pl.ds(hint(t * SEGMENTS, SEGMENTS), SEGMENTS)
        back = pl.ds(t, SEGMENTS, stride=seg)
        state = (cd0[at, :] + ca0[at, :] * f_enter) + (cd1[at, :] + ca1[at, :] * b_enter)
        conv_s[back, :] = state
        return 0

    lax.fori_loop(0, seg, join_body, 0, unroll=8)

    def mix_body(n, _):
        at = pl.ds(hint(n * rows, rows), rows)
        mixed[at, :] = (conv_s[at, :] * xpad[at, :]).astype(BF16)
        return 0

    lax.fori_loop(0, seq // rows, mix_body, 0)
    poll()

    own_cols = pl.ds(hint(tp * chans, chans), chans)
    for i in range(1, n_tp):
        peer = lax.rem(tp + i, n_tp)
        pltpu.make_async_remote_copy(
            src_ref=mixed.at[pl.ds(hint(peer * rows, rows), rows), :],
            dst_ref=tokb.at[:, own_cols],
            send_sem=tok_sem.at[0],
            recv_sem=tok_sem.at[1],
            device_id=(sp, peer),
            device_id_type=MESH,
        ).start()
    drains.append(lambda: blocked_all(tokb.at[:, 0 : (n_tp - 1) * chans], tok_sem.at[0]))
    tokb[:, own_cols] = mixed[pl.ds(own_rows, rows), :]
    poll()

    need(l_rt)
    need(l_wt)
    lane = lax.broadcasted_iota(jnp.int32, (n_sp, rows), 0)
    own_routes = jnp.where(core == 0, routv[:, 0:rows], routv[:, rows : 2 * rows])
    own_wts = jnp.where(core == 0, wtsv[:, 0:rows], wtsv[:, rows : 2 * rows])
    e0 = jnp.broadcast_to(own_routes[0:1, :], (n_sp, rows))
    e1 = jnp.broadcast_to(own_routes[1:2, :], (n_sp, rows))
    h0 = jnp.where(e0 == lane, 1.0, 0.0)
    h1 = jnp.where(e1 == lane, 1.0, 0.0)
    earlier = jnp.where(
        lax.broadcasted_iota(jnp.int32, (rows, rows), 0)
        < lax.broadcasted_iota(jnp.int32, (rows, rows), 1),
        1.0,
        0.0,
    )
    counts = jnp.dot(
        (h0 + h1).astype(BF16), earlier.astype(BF16), preferred_element_type=F32
    )
    slot0 = jnp.sum(counts * h0, axis=0, keepdims=True).astype(jnp.int32) + own_routes[
        0:1, :
    ] * cap
    slot1 = jnp.sum(counts * h1, axis=0, keepdims=True).astype(jnp.int32) + own_routes[
        1:2, :
    ] * cap
    slot_id = lax.broadcasted_iota(jnp.int32, (slots, rows), 0)
    hit0, hit1 = slot_id == slot0, slot_id == slot1
    sel = jnp.where(hit0 | hit1, 1.0, 0.0).astype(BF16)
    weights = jnp.where(hit0, own_wts[0:1, :], 0.0) + jnp.where(hit1, own_wts[1:2, :], 0.0)
    eye = jnp.where(
        lax.broadcasted_iota(jnp.int32, (rows, rows), 0)
        == lax.broadcasted_iota(jnp.int32, (rows, rows), 1),
        1.0,
        0.0,
    )
    table = lax.dot_general(
        eye,
        weights,
        (((1,), (1,)), ((), ())),
        precision=HIGHEST_MODE,
        preferred_element_type=F32,
    )
    high = table.astype(BF16)
    wtab[0] = high
    wtab[1] = (table - high.astype(F32)).astype(BF16)

    need(l_op)
    need(l_res)
    poll()
    blocked_all(tokb.at[:, 0 : (n_tp - 1) * chans], tok_sem.at[1])
    poll()
    pw = min(512, width)

    def proj_body(n, _):
        at = pl.ds(hint(n * pw, pw), pw)
        pbuf[:, at] = (
            jnp.dot(tokb[...], oproj[:, at], preferred_element_type=F32).astype(BF16).astype(F32)
        )
        return 0

    lax.fori_loop(0, width // pw, proj_body, 0)
    poll()

    def norm_body(n, _):
        at = pl.ds(hint(n * 16, 16), 16)
        v = pbuf[at, :]
        s = (residv[at, :].astype(F32) + v * root_mean(v) * gain[0:1, :]).astype(BF16).astype(F32)
        stream_s[at, :] = s
        normed[at, :] = (s * root_mean(s) * gain[1:2, :]).astype(BF16)
        return 0

    lax.fori_loop(0, rows // 16, norm_body, 0)
    poll()

    gw = min(256, width)

    def dispatch_body(n, _):
        at = pl.ds(hint(n * gw, gw), gw)
        outg[:, at] = jnp.dot(sel, normed[:, at], preferred_element_type=F32).astype(BF16)
        return 0

    lax.fori_loop(0, width // gw, dispatch_body, 0)
    poll()
    own_slots = pl.ds(hint(sp * cap, cap), cap)
    for i in range(1, n_sp):
        peer = lax.rem(sp + i, n_sp)
        pltpu.make_async_remote_copy(
            src_ref=outg.at[pl.ds(hint(peer * cap, cap), cap), :],
            dst_ref=arr.at[core, own_slots, :],
            send_sem=disp_send.at[0],
            recv_sem=disp_recv.at[i - 1],
            device_id=(peer, tp),
            device_id_type=MESH,
        ).start()

    drains.append(lambda: blocked_all(outg.at[0 : slots - cap, :], disp_send.at[0]))

    def forward(src_ref, at):
        pltpu.make_async_remote_copy(
            src_ref=src_ref,
            dst_ref=arr.at[core, at, :],
            send_sem=fwd_sem.at[0],
            recv_sem=fwd_sem.at[1],
            device_id=(sp, sibling),
            device_id_type=MESH,
        ).start()

    forward(outg.at[own_slots, :], own_slots)
    drains.append(lambda: blocked_all(outg, fwd_sem.at[0]))
    arr[core, own_slots, :] = outg[own_slots, :]
    poll()
    for i in range(1, n_sp):
        src = lax.rem(sp + n_sp - i, n_sp)
        at = pl.ds(hint(src * cap, cap), cap)
        blocked_all(arr.at[core, at, :], disp_recv.at[i - 1])
        forward(arr.at[core, at, :], at)
        poll()

    hidden_all = nz * hs
    hw = min(256, hidden_all)
    zh = hw // hs
    dims = (((1,), (1,)), ((), ()))

    def swap(c, k):
        at = hid.at[core, pl.ds(hint(c * slots, slots), slots), k * hw : (k + 1) * hw]
        return pltpu.make_async_remote_copy(
            src_ref=at,
            dst_ref=at,
            send_sem=hid_send.at[c, k],
            recv_sem=hid_recv.at[c, k],
            device_id=(sp, sibling),
            device_id_type=MESH,
        )

    def gate_block(c, k):
        x = arr[c]
        g, u = (
            lax.dot_general(
                x,
                w[k * zh : (k + 1) * zh].reshape(hw, width),
                dims,
                preferred_element_type=F32,
            )
            for w in (wg, wu)
        )
        hid[core, pl.ds(hint(c * slots, slots), slots), k * hw : (k + 1) * hw] = (
            g * jax.nn.sigmoid(g) * u
        ).astype(BF16)
        swap(c, k).start()
        drains.append(swap(c, k).wait_send)
        poll()

    need(l_wg)
    need(l_wu)
    blocks = hidden_all // hw
    for k in range(blocks):
        last = k == blocks - 1
        if last:
            poll()
        complete(0, zh * (k + 1))
        complete(1, zh * (k + 1))
        if last:
            poll()
        gate_block(core, k)
        if k == 0:
            blocked_all(arr.at[other], fwd_sem.at[1])
        gate_block(other, k)
    poll()
    for k in range(blocks):
        for c in range(2):
            swap(c, k).wait_recv()

    for q in range(CHUNKS):
        cols = slice(STARTS[q], STARTS[q] + WIDTHS[q])
        poll()
        poll()
        complete(2 + q)
        poll()

        hm = min(256, slots)

        def down_body(n, _):
            at = pl.ds(hint(n * hm, hm), hm)
            o = jnp.dot(
                hid[0, at, :], wd[0, :, cols], preferred_element_type=F32
            ) + jnp.dot(hid[1, at, :], wd[1, :, cols], preferred_element_type=F32)
            outb[q][at, :] = o.astype(BF16)
            return 0

        lax.fori_loop(0, 2 * slots // hm, down_body, 0)
        poll()
        for i in range(n_sp):
            peer = lax.rem(sp + i, n_sp)
            for mine in (1, 0):
                if i == 0 and mine:
                    continue
                c = core if mine else other
                pltpu.make_async_remote_copy(
                    src_ref=outb[q].at[pl.ds(hint(c * slots + peer * cap, cap), cap), :],
                    dst_ref=ret[q].at[core, own_slots, :],
                    send_sem=ret_send.at[q, mine],
                    recv_sem=ret_recv.at[q, mine],
                    device_id=(peer, tp if mine else sibling),
                    device_id_type=MESH,
                ).start()
        drains.append(
            lambda q=q: blocked_all(ret[q].at[core, 0 : slots - cap, :], ret_send.at[q, 1])
        )
        drains.append(lambda q=q: blocked_all(ret[q].at[other], ret_send.at[q, 0]))
        ret[q][core, own_slots, :] = outb[q][
            pl.ds(hint(core * slots + sp * cap, cap), cap), :
        ]
        poll()

    for q in range(CHUNKS):
        blocked_all(ret[q].at[core, 0 : slots - cap, :], ret_recv.at[q, 1])
        blocked_all(ret[q].at[other], ret_recv.at[q, 0])
        for c in range(2):
            v = ret[q][c]
            o = jnp.dot(wtab[0], v, preferred_element_type=F32) + jnp.dot(
                wtab[1], v, preferred_element_type=F32
            )
            at = c * half + STARTS[q]
            pbuf[:, at : at + WIDTHS[q]] = o.astype(BF16).astype(F32)

    def final_body(n, _):
        at = pl.ds(hint(n * 16, 16), 16)
        v = pbuf[at, :]
        out_ref[at, :] = (stream_s[at, :] + v * root_mean(v) * gain[2:3, :]).astype(BF16)
        return 0

    lax.fori_loop(0, rows // 16, final_body, 0)

    finish()


def on_device(
    mix_in,
    gate_in,
    conv_w,
    conv_b,
    decay_param,
    recur_gate,
    recur_bias,
    input_gate,
    input_bias,
    residual,
    out_proj,
    norm_gain,
    routes,
    route_wt,
    exp_gate,
    exp_up,
    exp_down,
):
    n_sp, n_tp = lax.axis_size("sp"), lax.axis_size("tp")
    nz = n_tp // 2
    seq, chans = mix_in.shape
    rows, width = residual.shape
    top = routes.shape[1]
    experts = n_sp * exp_gate.shape[0]
    cap = 2 * rows * top // experts
    slots = experts * cap
    hs = exp_gate.shape[2]
    half = width // 2
    far = nz // 2
    pieces = 2 + CHUNKS

    anywhere = pl.BlockSpec(memory_space=pltpu.HBM)
    onchip = pl.BlockSpec(memory_space=pltpu.VMEM)
    dma = pltpu.SemaphoreType.DMA
    scratch = [
        pltpu.VMEM((seq, chans), BF16),
        pltpu.VMEM((seq, chans), BF16),
        pltpu.VMEM((rows, width), BF16),
        pltpu.VMEM(out_proj.shape, BF16),
        pltpu.VMEM((top, 2 * rows), jnp.int32),
        pltpu.VMEM((top, 2 * rows), F32),
        pltpu.VMEM((2, 16, chans), BF16),
        pltpu.VMEM((seq + 16, chans), F32),
        pltpu.VMEM((seq, chans), F32),
        pltpu.VMEM((chans, 4 * chans), F32),
        pltpu.VMEM((seq, chans), F32),
        pltpu.VMEM((seq, chans), F32),
        pltpu.VMEM((seq, chans), F32),
        pltpu.VMEM((seq, chans), F32),
        pltpu.VMEM((n_sp, 8, chans), F32),
        pltpu.VMEM((seq, chans), BF16),
        pltpu.VMEM((rows, n_tp * chans), BF16),
        pltpu.VMEM((rows, width), F32),
        pltpu.VMEM((rows, width), F32),
        pltpu.VMEM((rows, width), BF16),
        pltpu.VMEM((slots, width), BF16),
        pltpu.VMEM((2, slots, width), BF16),
        pltpu.VMEM((nz, hs, width), BF16),
        pltpu.VMEM((nz, hs, width), BF16),
        pltpu.VMEM((2, nz * hs, half), BF16),
        pltpu.VMEM((2, 2 * slots, nz * hs), BF16),
        [pltpu.VMEM((2 * slots, w), BF16) for w in WIDTHS],
        [pltpu.VMEM((2, slots, w), BF16) for w in WIDTHS],
        pltpu.VMEM((2, rows, slots), BF16),
        dma((9,)),
        dma((2,)),
        dma((2,)),
        dma((2,)),
        dma((2,)),
        dma((1,)),
        dma((n_sp - 1,)),
        dma((2,)),
        dma((2, nz * hs // min(256, nz * hs))),
        dma((2, nz * hs // min(256, nz * hs))),
        dma((2,)),
        dma((2, pieces, far)),
        dma((2, pieces, far)),
        dma((CHUNKS, 2)),
        dma((CHUNKS, 2)),
    ]
    where = [
        anywhere,
        anywhere,
        onchip,
        onchip,
        onchip,
        onchip,
        onchip,
        onchip,
        onchip,
        anywhere,
        anywhere,
        onchip,
        anywhere,
        anywhere,
        anywhere,
        anywhere,
        anywhere,
    ]
    return pl.pallas_call(
        functools.partial(kernel, n_sp, n_tp),
        out_shape=jax.ShapeDtypeStruct((rows, width), BF16),
        in_specs=where,
        out_specs=onchip,
        scratch_shapes=scratch,
        compiler_params=pltpu.CompilerParams(
            collective_id=0, has_side_effects=True, vmem_limit_bytes=60 * 1024 * 1024
        ),
    )(
        mix_in,
        gate_in,
        conv_w,
        conv_b.reshape(1, chans),
        decay_param,
        recur_gate,
        recur_bias,
        input_gate,
        input_bias,
        residual,
        out_proj,
        norm_gain,
        routes.T,
        route_wt.T,
        exp_gate[0].T,
        exp_up[0].T,
        exp_down[0],
    )


def solution(mesh):
    return jax.shard_map(
        on_device,
        mesh=mesh,
        in_specs=(
            P("sp", "tp"),
            P("sp", "tp"),
            P(None, "tp"),
            P("tp"),
            P(None, "tp"),
            P(None, "tp", None, None),
            P(None, "tp"),
            P(None, "tp", None, None),
            P(None, "tp"),
            P(("sp", "tp"), None),
            P(),
            P(),
            P("sp", None),
            P("sp", None),
            P("sp", None, "tp"),
            P("sp", None, "tp"),
            P("sp", "tp", None),
        ),
        out_specs=P(("sp", "tp"), None),
        check_vma=False,
    )
```

```python
import functools

import jax
import jax.numpy as jnp
from jax import lax
from jax.experimental import pallas as pl
from jax.experimental.pallas import tpu as pltpu
from jax.sharding import PartitionSpec as P

EPSILON = 1e-06
HIGHEST_MODE = lax.Precision.HIGHEST
MESH = pl.DeviceIdType.MESH
F32, BF16 = jnp.float32, jnp.bfloat16
SEGMENTS = 8
WIDTHS = (128, 128, 128, 128, 256, 256)
CHUNKS = len(WIDTHS)
NEVER = 1 << 20
PLAN = (
    ((0, 0, 1), (0, 1, 1), (1, 1, 1), (1, 0, 1),),
    (),
    ((0, 4, 1), (0, 5, 1), (0, 2, 1), (0, 3, 1), (1, 4, 1), (1, 5, 1), (1, 2, 1), (1, 3, 1),),
    (),
    (),
    (),
    ((0, 0, 2), (1, 1, 2),),
    (),
    ((0, 1, 2), (1, 0, 2), (0, 0, 3), (1, 2, 2), (1, 1, 3),),
    (),
    (),
    (),
    (),
    (),
    ((0, 2, 2), (0, 3, 2), (0, 4, 2), (0, 5, 2), (0, 6, 1), (1, 3, 2), (1, 4, 2), (1, 5, 2), (1, 6, 1), (0, 1, 3), (1, 7, 1), (1, 2, 3),),
    (),
    ((1, 0, 3),),
    (),
    (),
    (),
    (),
    ((0, 2, 3),),
    ((0, 3, 3), (1, 3, 3),),
    (),
    (),
    ((0, 0, 4), (1, 1, 4),),
    (),
    (),
    (),
    (),
    ((0, 6, 2), (0, 7, 1), (0, 4, 3), (1, 6, 2), (1, 7, 2),),
    (),
    ((0, 2, 4), (1, 3, 4),),
    ((0, 6, 3), (1, 4, 3),),
    ((1, 5, 3),),
    ((0, 4, 4), (1, 6, 3),),
    ((0, 7, 2),),
    (),
    (),
    (),
    ((1, 7, 3),),
    (),
    (),
    (),
    ((0, 5, 3),),
    (),
    (),
    (),
    ((0, 6, 4), (1, 5, 4),),
    (),
    (),
    (),
    (),
    ((0, 7, 3), (1, 7, 4),),
    (),
    (),
    (),
    (),
    (),
    (),
    (),
    (),
    (),
    (),
    (),
    (),
)
STARTS = tuple(sum(WIDTHS[:k]) for k in range(CHUNKS))


def hint(value, step):
    return pl.multiple_of(value, step)


def blocked_all(copy_ref, sem):
    pltpu.make_async_copy(copy_ref, copy_ref, sem).wait()


def root_mean(values):
    return lax.rsqrt(jnp.mean(values * values, axis=-1, keepdims=True) + EPSILON)


def places(nz):
    order = [0]
    for step in range(1, nz // 2 + 1):
        order += [step, nz - step] if step < nz - step else [step]
    return {distance: place for place, distance in enumerate(order)}


def kernel(
    n_sp,
    n_tp,
    mix_h,
    gate_h,
    conv_w,
    conv_b,
    decay,
    rg,
    rb,
    ig,
    ib,
    resid_h,
    oproj_h,
    gain,
    routes_h,
    wts_h,
    wg_h,
    wu_h,
    wd_h,
    out_ref,
    mixv,
    gatev,
    residv,
    oproj,
    routv,
    wtsv,
    halo,
    xpad,
    conv_s,
    wcat,
    ca0,
    cd0,
    ca1,
    cd1,
    stats,
    mixed,
    tokb,
    pbuf,
    stream_s,
    normed,
    outg,
    arr,
    wg,
    wu,
    wd,
    hid,
    outb,
    ret,
    wtab,
    known,
    load_sem,
    halo_send,
    halo_recv,
    stat_sem,
    tok_sem,
    disp_send,
    disp_recv,
    fwd_sem,
    hid_send,
    hid_recv,
    pre_sem,
    ring_send,
    ring_recv,
    ret_send,
    ret_recv,
):
    nz = n_tp // 2
    sp, tp = lax.axis_index("sp"), lax.axis_index("tp")
    z, core = tp // 2, lax.rem(tp, 2)
    other = 1 - core
    sibling = 2 * z + other
    seq, chans = mix_h.shape
    rows, width = resid_h.shape
    half = width // 2
    hs = wg_h.shape[0]
    cap = outg.shape[0] // n_sp
    slots = n_sp * cap
    seg = seq // SEGMENTS

    loads = {}
    drains = []

    def load(src, dst, k):
        copy = pltpu.make_async_copy(src, dst, load_sem.at[k])
        copy.start()
        loads[k] = copy
        return k

    def need(k):
        if k in loads:
            loads.pop(k).wait()

    own_rows = hint(tp * rows, rows)
    l_mix = load(mix_h, mixv, 0)
    l_gate = load(gate_h, gatev, 1)
    l_wg = load(wg_h, wg.at[0], 2)
    l_wu = load(wu_h, wu.at[0], 3)
    l_wd = load(
        wd_h.at[:, pl.ds(hint(core * half, half), half)],
        wd.at[core, 0:hs, :],
        4,
    )
    l_op = load(oproj_h, oproj, 5)
    l_res = load(resid_h, residv, 6)
    pair = pl.ds(hint(z * 2 * rows, 2 * rows), 2 * rows)
    l_rt = load(routes_h.at[:, pair], routv, 7)
    l_wt = load(wts_h.at[:, pair], wtsv, 8)

    barrier = pltpu.get_barrier_semaphore()
    side = 4
    x, y = lax.rem(sp, side), sp // side
    near_by = [(sp, sibling)]
    near_by += [(sp, lax.rem(tp + n_tp + 2 * step, n_tp)) for step in (1, -1)]
    near_by += [(y * side + lax.rem(x + side + step, side), tp) for step in (1, -1)]
    near_by += [(lax.rem(sp + n_sp + side * step, n_sp), tp) for step in (1, -1)]
    partners = near_by + [(lax.rem(sp + n_sp + step, n_sp), tp) for step in (1, -1)]
    for peer in partners:
        pl.semaphore_signal(barrier, inc=1, device_id=peer, device_id_type=MESH)

    heads, hd = rg.shape[1], rg.shape[2]
    wcat[...] = jnp.zeros_like(wcat)
    for d in range(2):
        for which, ref in enumerate((rg, ig)):
            for h in range(heads):
                at = (2 * d + which) * chans + h * hd
                wcat[h * hd : (h + 1) * hd, at : at + hd] = ref[d, h]

    need(l_mix)

    xpad[0:8, :] = jnp.zeros((8, chans), F32)
    xpad[8 : 8 + seq, :] = mixv[...].astype(F32)
    xpad[8 + seq : 16 + seq, :] = jnp.zeros((8, chans), F32)

    def strided(t):
        return xpad[pl.ds(t, SEGMENTS, stride=seg), :]

    taps = [jnp.broadcast_to(conv_w[j : j + 1, :], (SEGMENTS, chans)) for j in range(4)]
    bias = jnp.broadcast_to(conv_b[0:1, :], (SEGMENTS, chans))

    def weigh(x0, x1, x2, x3):
        return bias + x0 * taps[0] + x1 * taps[1] + x2 * taps[2] + x3 * taps[3]

    def conv_body(t, window):
        x0, x1, x2 = window
        x3 = strided(9 + t)
        conv_s[pl.ds(hint(t * SEGMENTS, SEGMENTS), SEGMENTS), :] = weigh(x0, x1, x2, x3)
        return x1, x2, x3

    lax.fori_loop(0, seg, conv_body, (strided(6), strided(7), strided(8)), unroll=8)

    pl.semaphore_wait(barrier, len(partners))

    def tell(k):
        for peer in near_by:
            pl.semaphore_signal(known.at[k], inc=1, device_id=peer, device_id_type=MESH)

    def hear(k):
        pl.semaphore_wait(known.at[k], len(near_by))

    tell(0)

    right = 2 * lax.rem(z + 1, nz) + core
    left = 2 * lax.rem(z + nz - 1, nz) + core

    far, near = nz // 2, nz - 1 - nz // 2
    place = places(nz)

    def hops(direction, piece):
        return far if piece % 2 == direction else near

    def piece_ref(direction, piece, hop):
        at = place[hop if direction == 1 or hop == 0 else nz - hop]
        if piece < 2:
            return (wg, wu)[piece].at[at]
        q = piece - 2
        return wd.at[:, at * hs : (at + 1) * hs, STARTS[q] : STARTS[q] + WIDTHS[q]]

    def ring_copy(direction, piece, hop):
        src = piece_ref(direction, piece, hop - 1)
        if hop == 1 and piece < 2:
            src = (wg_h, wu_h)[piece]
        return pltpu.make_async_remote_copy(
            src_ref=src,
            dst_ref=piece_ref(direction, piece, hop),
            send_sem=ring_send.at[direction, piece, hop - 1],
            recv_sem=ring_recv.at[direction, piece, hop - 1],
            device_id=(sp, right if direction == 0 else left),
            device_id_type=MESH,
        )

    sent = []
    taken = set()
    stage = [0]

    def take(direction, piece, hop):
        if (direction, piece, hop) not in taken:
            taken.add((direction, piece, hop))
            blocked_all(
                piece_ref(direction, piece, hop), ring_recv.at[direction, piece, hop - 1]
            )

    def poll():
        for direction, piece, hop in PLAN[stage[0]]:
            if hop > 1:
                take(direction, piece, hop - 1)
            elif piece >= 2 and "pre" not in taken:
                taken.add("pre")
                need(l_wd)
                pre.wait()
            ring_copy(direction, piece, hop).start()
            sent.append((direction, piece, hop))
        stage[0] += 1

    def complete(piece, end=NEVER):
        for direction in (0, 1):
            for hop in range(1, hops(direction, piece) + 1):
                if place[hop if direction == 1 else nz - hop] < end:
                    assert (direction, piece, hop) in sent
                    take(direction, piece, hop)

    def finish():
        for drain in drains:
            drain()
        for event in sent:
            ring_copy(*event).wait_send()

    nxt, prv = lax.rem(sp + 1, n_sp), lax.rem(sp + n_sp - 1, n_sp)
    hr = halo.shape[1]
    to_next = pltpu.make_async_remote_copy(
        src_ref=mixv.at[seq - hr : seq, :],
        dst_ref=halo.at[0],
        send_sem=halo_send.at[0],
        recv_sem=halo_recv.at[0],
        device_id=(nxt, tp),
        device_id_type=MESH,
    )
    to_prev = pltpu.make_async_remote_copy(
        src_ref=mixv.at[0:hr, :],
        dst_ref=halo.at[1],
        send_sem=halo_send.at[1],
        recv_sem=halo_recv.at[1],
        device_id=(prv, tp),
        device_id_type=MESH,
    )
    to_next.start()
    to_prev.start()

    pre = pltpu.make_async_remote_copy(
        src_ref=wd_h.at[:, pl.ds(hint(other * half, half), half)],
        dst_ref=wd.at[core, 0:hs, :],
        send_sem=pre_sem.at[0],
        recv_sem=pre_sem.at[1],
        device_id=(sp, sibling),
        device_id_type=MESH,
    )
    poll()
    pre.start()

    rates = []
    for d in range(2):
        x = -decay[d : d + 1, :]
        rates.append(-8.0 * (jnp.maximum(x, 0.0) + jnp.log1p(jnp.exp(-jnp.abs(x)))))
    part = 128

    def coefficients(c):
        pre_act = jnp.dot(c, wcat[...], precision=HIGHEST_MODE, preferred_element_type=F32)
        found = []
        for d in range(2):
            r = jax.nn.sigmoid(pre_act[:, 2 * d * chans : (2 * d + 1) * chans] + rb[d : d + 1, :])
            i = jax.nn.sigmoid(
                pre_act[:, (2 * d + 1) * chans : (2 * d + 2) * chans] + ib[d : d + 1, :]
            )
            la = r * rates[d]
            a = jnp.exp(la)
            x = 2.0 * la
            series = 1.0 + x * (1.0 / 6.0)
            for k in (5.0, 4.0, 3.0, 2.0):
                series = 1.0 + x * (1.0 / k) * series
            gap = jnp.where(x > -0.3, -x * series, 1.0 - a * a)
            found += [a, jnp.sqrt(gap) * (i * c)]
        return found

    kept = (ca0, cd0, ca1, cd1)

    def coef_body(n, _):
        at = pl.ds(hint(n * part, part), part)
        for ref, value in zip(kept, coefficients(conv_s[at, :])):
            ref[at, :] = value
        return 0

    lax.fori_loop(0, seq // part // 2, coef_body, 0)
    hear(0)
    tell(1)
    poll()
    lax.fori_loop(seq // part // 2, seq // part, coef_body, 0)
    hear(1)
    tell(2)

    poll()
    to_next.wait()
    to_prev.wait()
    before = jnp.where(sp > 0, 1.0, 0.0).astype(F32)
    after = jnp.where(sp < n_sp - 1, 1.0, 0.0).astype(F32)
    xpad[0:8, :] = halo[0].astype(F32)[hr - 8 : hr] * before
    xpad[8 + seq : 16 + seq, :] = halo[1].astype(F32)[0:8] * after
    ends = jnp.concatenate(
        [weigh(*(strided(6 + t + j) for j in range(4))) for t in (0, 1, seg - 1)], axis=0
    )
    for ref, value in zip(kept, coefficients(ends)):
        ref[0 : 2 * SEGMENTS, :] = value[0 : 2 * SEGMENTS]
        ref[seq - SEGMENTS : seq, :] = value[2 * SEGMENTS :]

    zero = jnp.zeros((SEGMENTS, chans), F32)
    one = jnp.ones((SEGMENTS, chans), F32)

    def scan_body(t, carry):
        f, p, g, q = carry
        fat = pl.ds(hint(t * SEGMENTS, SEGMENTS), SEGMENTS)
        bat = pl.ds(hint((seg - 1 - t) * SEGMENTS, SEGMENTS), SEGMENTS)
        a, b = ca0[fat, :], ca1[bat, :]
        f = a * f + cd0[fat, :]
        p = a * p
        g = b * g + cd1[bat, :]
        q = b * q
        cd0[fat, :] = f
        ca0[fat, :] = p
        cd1[bat, :] = g
        ca1[bat, :] = q
        return f, p, g, q

    f_end, p_end, g_end, q_end = lax.fori_loop(0, seg, scan_body, (zero, one, zero, one), unroll=8)

    poll()
    hear(2)
    tell(3)

    row = lambda v, k: v[k : k + 1, :]
    f_scale, f_shift = [row(one, 0)], [row(zero, 0)]
    for k in range(SEGMENTS):
        f_scale.append(row(p_end, k) * f_scale[-1])
        f_shift.append(row(p_end, k) * f_shift[-1] + row(f_end, k))
    b_scale, b_shift = [row(one, 0)], [row(zero, 0)]
    for k in range(SEGMENTS - 1, -1, -1):
        b_scale.append(row(q_end, k) * b_scale[-1])
        b_shift.append(row(q_end, k) * b_shift[-1] + row(g_end, k))
    for k, v in enumerate((f_scale[-1], f_shift[-1], b_scale[-1], b_shift[-1])):
        stats[sp, k : k + 1, :] = v
    for i in range(1, n_sp):
        pltpu.make_async_remote_copy(
            src_ref=stats.at[sp],
            dst_ref=stats.at[sp],
            send_sem=stat_sem.at[0],
            recv_sem=stat_sem.at[1],
            device_id=(lax.rem(sp + i, n_sp), tp),
            device_id_type=MESH,
        ).start()
    drains.append(lambda: blocked_all(stats.at[0 : n_sp - 1], stat_sem.at[0]))
    poll()

    need(l_gate)

    def gelu_body(n, _):
        at = pl.ds(hint(n * 64, 64), 64)
        xpad[at, :] = jax.nn.gelu(gatev[at, :].astype(F32))
        return 0

    lax.fori_loop(0, seq // 64, gelu_body, 0)
    poll()
    blocked_all(stats.at[0 : n_sp - 1], stat_sem.at[1])

    f_in = jnp.zeros((1, chans), F32)
    b_in = jnp.zeros((1, chans), F32)
    for j in range(n_sp):
        f_in = jnp.where(j < sp, stats[j, 0:1, :] * f_in + stats[j, 1:2, :], f_in)
        k = n_sp - 1 - j
        b_in = jnp.where(k > sp, stats[k, 2:3, :] * b_in + stats[k, 3:4, :], b_in)
    f_enter = jnp.concatenate(
        [f_scale[k] * f_in + f_shift[k] for k in range(SEGMENTS)], axis=0
    )
    b_enter = jnp.concatenate(
        [b_scale[SEGMENTS - 1 - k] * b_in + b_shift[SEGMENTS - 1 - k] for k in range(SEGMENTS)],
        axis=0,
    )

    def join_body(t, _):
        at = pl.ds(hint(t * SEGMENTS, SEGMENTS), SEGMENTS)
        back = pl.ds(t, SEGMENTS, stride=seg)
        state = (cd0[at, :] + ca0[at, :] * f_enter) + (cd1[at, :] + ca1[at, :] * b_enter)
        conv_s[back, :] = state
        return 0

    lax.fori_loop(0, seg, join_body, 0, unroll=8)

    def mix_body(n, _):
        at = pl.ds(hint(n * rows, rows), rows)
        mixed[at, :] = (conv_s[at, :] * xpad[at, :]).astype(BF16)
        return 0

    lax.fori_loop(0, seq // rows, mix_body, 0)
    poll()

    hear(3)
    own_cols = pl.ds(hint(tp * chans, chans), chans)
    for i in range(1, n_tp):
        peer = lax.rem(tp + i, n_tp)
        pltpu.make_async_remote_copy(
            src_ref=mixed.at[pl.ds(hint(peer * rows, rows), rows), :],
            dst_ref=tokb.at[:, own_cols],
            send_sem=tok_sem.at[0],
            recv_sem=tok_sem.at[1],
            device_id=(sp, peer),
            device_id_type=MESH,
        ).start()
    drains.append(lambda: blocked_all(tokb.at[:, 0 : (n_tp - 1) * chans], tok_sem.at[0]))
    tokb[:, own_cols] = mixed[pl.ds(own_rows, rows), :]
    poll()

    need(l_rt)
    need(l_wt)
    lane = lax.broadcasted_iota(jnp.int32, (n_sp, rows), 0)
    own_routes = jnp.where(core == 0, routv[:, 0:rows], routv[:, rows : 2 * rows])
    own_wts = jnp.where(core == 0, wtsv[:, 0:rows], wtsv[:, rows : 2 * rows])
    e0 = jnp.broadcast_to(own_routes[0:1, :], (n_sp, rows))
    e1 = jnp.broadcast_to(own_routes[1:2, :], (n_sp, rows))
    h0 = jnp.where(e0 == lane, 1.0, 0.0)
    h1 = jnp.where(e1 == lane, 1.0, 0.0)
    earlier = jnp.where(
        lax.broadcasted_iota(jnp.int32, (rows, rows), 0)
        < lax.broadcasted_iota(jnp.int32, (rows, rows), 1),
        1.0,
        0.0,
    )
    counts = jnp.dot(
        (h0 + h1).astype(BF16), earlier.astype(BF16), preferred_element_type=F32
    )
    slot0 = jnp.sum(counts * h0, axis=0, keepdims=True).astype(jnp.int32) + own_routes[
        0:1, :
    ] * cap
    slot1 = jnp.sum(counts * h1, axis=0, keepdims=True).astype(jnp.int32) + own_routes[
        1:2, :
    ] * cap
    slot_id = lax.broadcasted_iota(jnp.int32, (slots, rows), 0)
    hit0, hit1 = slot_id == slot0, slot_id == slot1
    sel = jnp.where(hit0 | hit1, 1.0, 0.0).astype(BF16)
    weights = jnp.where(hit0, own_wts[0:1, :], 0.0) + jnp.where(hit1, own_wts[1:2, :], 0.0)
    eye = jnp.where(
        lax.broadcasted_iota(jnp.int32, (rows, rows), 0)
        == lax.broadcasted_iota(jnp.int32, (rows, rows), 1),
        1.0,
        0.0,
    )
    table = lax.dot_general(
        eye,
        weights,
        (((1,), (1,)), ((), ())),
        precision=HIGHEST_MODE,
        preferred_element_type=F32,
    )
    high = table.astype(BF16)
    wtab[0] = high
    wtab[1] = (table - high.astype(F32)).astype(BF16)

    need(l_op)
    need(l_res)
    poll()
    blocked_all(tokb.at[:, 0 : (n_tp - 1) * chans], tok_sem.at[1])
    poll()
    pw = min(512, width)

    def proj_body(n, _):
        at = pl.ds(hint(n * pw, pw), pw)
        pbuf[:, at] = (
            jnp.dot(tokb[...], oproj[:, at], preferred_element_type=F32).astype(BF16).astype(F32)
        )
        return 0

    lax.fori_loop(0, width // pw, proj_body, 0)
    poll()

    def norm_body(n, _):
        at = pl.ds(hint(n * 16, 16), 16)
        v = pbuf[at, :]
        s = (residv[at, :].astype(F32) + v * root_mean(v) * gain[0:1, :]).astype(BF16).astype(F32)
        stream_s[at, :] = s
        normed[at, :] = (s * root_mean(s) * gain[1:2, :]).astype(BF16)
        return 0

    lax.fori_loop(0, rows // 16, norm_body, 0)
    poll()

    gw = min(256, width)

    def dispatch_body(n, _):
        at = pl.ds(hint(n * gw, gw), gw)
        outg[:, at] = jnp.dot(sel, normed[:, at], preferred_element_type=F32).astype(BF16)
        return 0

    lax.fori_loop(0, width // gw, dispatch_body, 0)
    poll()
    own_slots = pl.ds(hint(sp * cap, cap), cap)
    for i in range(1, n_sp):
        peer = lax.rem(sp + i, n_sp)
        pltpu.make_async_remote_copy(
            src_ref=outg.at[pl.ds(hint(peer * cap, cap), cap), :],
            dst_ref=arr.at[core, own_slots, :],
            send_sem=disp_send.at[0],
            recv_sem=disp_recv.at[i - 1],
            device_id=(peer, tp),
            device_id_type=MESH,
        ).start()

    drains.append(lambda: blocked_all(outg.at[0 : slots - cap, :], disp_send.at[0]))

    def forward(src_ref, at):
        pltpu.make_async_remote_copy(
            src_ref=src_ref,
            dst_ref=arr.at[core, at, :],
            send_sem=fwd_sem.at[0],
            recv_sem=fwd_sem.at[1],
            device_id=(sp, sibling),
            device_id_type=MESH,
        ).start()

    forward(outg.at[own_slots, :], own_slots)
    drains.append(lambda: blocked_all(outg, fwd_sem.at[0]))
    arr[core, own_slots, :] = outg[own_slots, :]
    poll()
    for i in range(1, n_sp):
        src = lax.rem(sp + n_sp - i, n_sp)
        at = pl.ds(hint(src * cap, cap), cap)
        blocked_all(arr.at[core, at, :], disp_recv.at[i - 1])
        forward(arr.at[core, at, :], at)
        poll()

    hidden_all = nz * hs
    hw = min(256, hidden_all)
    zh = hw // hs
    dims = (((1,), (1,)), ((), ()))

    def swap(c, k):
        at = hid.at[core, pl.ds(hint(c * slots, slots), slots), k * hw : (k + 1) * hw]
        return pltpu.make_async_remote_copy(
            src_ref=at,
            dst_ref=at,
            send_sem=hid_send.at[c, k],
            recv_sem=hid_recv.at[c, k],
            device_id=(sp, sibling),
            device_id_type=MESH,
        )

    def gate_block(c, k):
        x = arr[c]
        g, u = (
            lax.dot_general(
                x,
                w[k * zh : (k + 1) * zh].reshape(hw, width),
                dims,
                preferred_element_type=F32,
            )
            for w in (wg, wu)
        )
        hid[core, pl.ds(hint(c * slots, slots), slots), k * hw : (k + 1) * hw] = (
            g * jax.nn.sigmoid(g) * u
        ).astype(BF16)
        swap(c, k).start()
        drains.append(swap(c, k).wait_send)
        poll()

    need(l_wg)
    need(l_wu)
    blocks = hidden_all // hw
    for k in range(blocks):
        last = k == blocks - 1
        if last:
            poll()
        complete(0, zh * (k + 1))
        complete(1, zh * (k + 1))
        if last:
            poll()
        gate_block(core, k)
        if k == 0:
            blocked_all(arr.at[other], fwd_sem.at[1])
        gate_block(other, k)
    poll()
    for k in range(blocks):
        for c in range(2):
            swap(c, k).wait_recv()

    for q in range(CHUNKS):
        cols = slice(STARTS[q], STARTS[q] + WIDTHS[q])
        poll()
        poll()
        complete(2 + q)
        poll()

        hm = min(256, slots)

        def down_body(n, _):
            at = pl.ds(hint(n * hm, hm), hm)
            o = jnp.dot(
                hid[0, at, :], wd[0, :, cols], preferred_element_type=F32
            ) + jnp.dot(hid[1, at, :], wd[1, :, cols], preferred_element_type=F32)
            outb[q][at, :] = o.astype(BF16)
            return 0

        lax.fori_loop(0, 2 * slots // hm, down_body, 0)
        poll()
        for i in range(n_sp):
            peer = lax.rem(sp + i, n_sp)
            for mine in (1, 0):
                if i == 0 and mine:
                    continue
                c = core if mine else other
                pltpu.make_async_remote_copy(
                    src_ref=outb[q].at[pl.ds(hint(c * slots + peer * cap, cap), cap), :],
                    dst_ref=ret[q].at[core, own_slots, :],
                    send_sem=ret_send.at[q, mine],
                    recv_sem=ret_recv.at[q, mine],
                    device_id=(peer, tp if mine else sibling),
                    device_id_type=MESH,
                ).start()
        drains.append(
            lambda q=q: blocked_all(ret[q].at[core, 0 : slots - cap, :], ret_send.at[q, 1])
        )
        drains.append(lambda q=q: blocked_all(ret[q].at[other], ret_send.at[q, 0]))
        ret[q][core, own_slots, :] = outb[q][
            pl.ds(hint(core * slots + sp * cap, cap), cap), :
        ]
        poll()

    for q in range(CHUNKS):
        blocked_all(ret[q].at[core, 0 : slots - cap, :], ret_recv.at[q, 1])
        blocked_all(ret[q].at[other], ret_recv.at[q, 0])
        for c in range(2):
            v = ret[q][c]
            o = jnp.dot(wtab[0], v, preferred_element_type=F32) + jnp.dot(
                wtab[1], v, preferred_element_type=F32
            )
            at = c * half + STARTS[q]
            pbuf[:, at : at + WIDTHS[q]] = o.astype(BF16).astype(F32)

    def final_body(n, _):
        at = pl.ds(hint(n * 16, 16), 16)
        v = pbuf[at, :]
        out_ref[at, :] = (stream_s[at, :] + v * root_mean(v) * gain[2:3, :]).astype(BF16)
        return 0

    lax.fori_loop(0, rows // 16, final_body, 0)

    finish()


def on_device(
    mix_in,
    gate_in,
    conv_w,
    conv_b,
    decay_param,
    recur_gate,
    recur_bias,
    input_gate,
    input_bias,
    residual,
    out_proj,
    norm_gain,
    routes,
    route_wt,
    exp_gate,
    exp_up,
    exp_down,
):
    n_sp, n_tp = lax.axis_size("sp"), lax.axis_size("tp")
    nz = n_tp // 2
    seq, chans = mix_in.shape
    rows, width = residual.shape
    top = routes.shape[1]
    experts = n_sp * exp_gate.shape[0]
    cap = 2 * rows * top // experts
    slots = experts * cap
    hs = exp_gate.shape[2]
    half = width // 2
    far = nz // 2
    pieces = 2 + CHUNKS

    anywhere = pl.BlockSpec(memory_space=pltpu.HBM)
    onchip = pl.BlockSpec(memory_space=pltpu.VMEM)
    dma = pltpu.SemaphoreType.DMA
    scratch = [
        pltpu.VMEM((seq, chans), BF16),
        pltpu.VMEM((seq, chans), BF16),
        pltpu.VMEM((rows, width), BF16),
        pltpu.VMEM(out_proj.shape, BF16),
        pltpu.VMEM((top, 2 * rows), jnp.int32),
        pltpu.VMEM((top, 2 * rows), F32),
        pltpu.VMEM((2, 16, chans), BF16),
        pltpu.VMEM((seq + 16, chans), F32),
        pltpu.VMEM((seq, chans), F32),
        pltpu.VMEM((chans, 4 * chans), F32),
        pltpu.VMEM((seq, chans), F32),
        pltpu.VMEM((seq, chans), F32),
        pltpu.VMEM((seq, chans), F32),
        pltpu.VMEM((seq, chans), F32),
        pltpu.VMEM((n_sp, 8, chans), F32),
        pltpu.VMEM((seq, chans), BF16),
        pltpu.VMEM((rows, n_tp * chans), BF16),
        pltpu.VMEM((rows, width), F32),
        pltpu.VMEM((rows, width), F32),
        pltpu.VMEM((rows, width), BF16),
        pltpu.VMEM((slots, width), BF16),
        pltpu.VMEM((2, slots, width), BF16),
        pltpu.VMEM((nz, hs, width), BF16),
        pltpu.VMEM((nz, hs, width), BF16),
        pltpu.VMEM((2, nz * hs, half), BF16),
        pltpu.VMEM((2, 2 * slots, nz * hs), BF16),
        [pltpu.VMEM((2 * slots, w), BF16) for w in WIDTHS],
        [pltpu.VMEM((2, slots, w), BF16) for w in WIDTHS],
        pltpu.VMEM((2, rows, slots), BF16),
        pltpu.SemaphoreType.REGULAR((4,)),
        dma((9,)),
        dma((2,)),
        dma((2,)),
        dma((2,)),
        dma((2,)),
        dma((1,)),
        dma((n_sp - 1,)),
        dma((2,)),
        dma((2, nz * hs // min(256, nz * hs))),
        dma((2, nz * hs // min(256, nz * hs))),
        dma((2,)),
        dma((2, pieces, far)),
        dma((2, pieces, far)),
        dma((CHUNKS, 2)),
        dma((CHUNKS, 2)),
    ]
    where = [
        anywhere,
        anywhere,
        onchip,
        onchip,
        onchip,
        onchip,
        onchip,
        onchip,
        onchip,
        anywhere,
        anywhere,
        onchip,
        anywhere,
        anywhere,
        anywhere,
        anywhere,
        anywhere,
    ]
    return pl.pallas_call(
        functools.partial(kernel, n_sp, n_tp),
        out_shape=jax.ShapeDtypeStruct((rows, width), BF16),
        in_specs=where,
        out_specs=onchip,
        scratch_shapes=scratch,
        compiler_params=pltpu.CompilerParams(
            collective_id=0, has_side_effects=True, vmem_limit_bytes=60 * 1024 * 1024
        ),
    )(
        mix_in,
        gate_in,
        conv_w,
        conv_b.reshape(1, chans),
        decay_param,
        recur_gate,
        recur_bias,
        input_gate,
        input_bias,
        residual,
        out_proj,
        norm_gain,
        routes.T,
        route_wt.T,
        exp_gate[0].T,
        exp_up[0].T,
        exp_down[0],
    )


def solution(mesh):
    return jax.shard_map(
        on_device,
        mesh=mesh,
        in_specs=(
            P("sp", "tp"),
            P("sp", "tp"),
            P(None, "tp"),
            P("tp"),
            P(None, "tp"),
            P(None, "tp", None, None),
            P(None, "tp"),
            P(None, "tp", None, None),
            P(None, "tp"),
            P(("sp", "tp"), None),
            P(),
            P(),
            P("sp", None),
            P("sp", None),
            P("sp", None, "tp"),
            P("sp", None, "tp"),
            P("sp", "tp", None),
        ),
        out_specs=P(("sp", "tp"), None),
        check_vma=False,
    )
```

```python
import functools

import jax
import jax.numpy as jnp
from jax import lax
from jax.experimental import pallas as pl
from jax.experimental.pallas import tpu as pltpu
from jax.sharding import PartitionSpec as P

EPSILON = 1e-06
HIGHEST_MODE = lax.Precision.HIGHEST
MESH = pl.DeviceIdType.MESH
F32, BF16 = jnp.float32, jnp.bfloat16
SEGMENTS = 8
WIDTHS = (128, 128, 128, 128, 256, 256)
CHUNKS = len(WIDTHS)
NEVER = 1 << 20
PLAN = (
    ((0, 0, 1), (0, 1, 1), (1, 1, 1), (1, 0, 1),),
    (),
    ((0, 2, 1), (0, 3, 1), (0, 4, 1), (0, 5, 1), (1, 2, 1), (1, 3, 1), (1, 4, 1), (1, 5, 1),),
    (),
    (),
    (),
    ((0, 0, 2), (1, 1, 2),),
    (),
    ((0, 1, 2), (1, 0, 2), (0, 4, 2), (0, 5, 2), (0, 2, 2), (0, 3, 2), (0, 0, 3), (1, 4, 2), (1, 5, 2), (1, 2, 2), (1, 3, 2), (1, 1, 3),),
    (),
    (),
    (),
    (),
    (),
    ((0, 6, 1), (1, 6, 1), (0, 1, 3), (1, 7, 1), (1, 0, 3),),
    (),
    (),
    (),
    ((0, 2, 3),),
    ((0, 3, 3),),
    ((1, 2, 3),),
    ((1, 3, 3),),
    (),
    ((0, 0, 4), (1, 1, 4),),
    (),
    (),
    (),
    (),
    (),
    (),
    ((0, 6, 2), (0, 7, 1), (0, 4, 3), (0, 5, 3), (1, 6, 2), (1, 7, 2), (1, 4, 3),),
    (),
    ((0, 2, 4), (1, 5, 3), (1, 3, 4),),
    ((0, 6, 3),),
    (),
    ((0, 7, 2), (1, 6, 3), (0, 4, 4),),
    (),
    (),
    ((1, 7, 3),),
    (),
    ((1, 5, 4),),
    (),
    (),
    (),
    (),
    ((0, 6, 4),),
    (),
    (),
    ((0, 7, 3),),
    (),
    (),
    (),
    (),
    ((1, 7, 4),),
    (),
    (),
    (),
    (),
    (),
    (),
    (),
    (),
    (),
    (),
    (),
    (),
)
STARTS = tuple(sum(WIDTHS[:k]) for k in range(CHUNKS))


def hint(value, step):
    return pl.multiple_of(value, step)


def blocked_all(copy_ref, sem):
    pltpu.make_async_copy(copy_ref, copy_ref, sem).wait()


def root_mean(values):
    return lax.rsqrt(jnp.mean(values * values, axis=-1, keepdims=True) + EPSILON)


def places(nz):
    order = [0]
    for step in range(1, nz // 2 + 1):
        order += [step, nz - step] if step < nz - step else [step]
    return {distance: place for place, distance in enumerate(order)}


def kernel(
    n_sp,
    n_tp,
    mix_h,
    gate_h,
    conv_w,
    conv_b,
    decay,
    rg,
    rb,
    ig,
    ib,
    resid_h,
    oproj_h,
    gain,
    routes_h,
    wts_h,
    wg_h,
    wu_h,
    wd_h,
    out_ref,
    mixv,
    gatev,
    residv,
    oproj,
    routv,
    wtsv,
    halo,
    xpad,
    conv_s,
    wcat,
    ca0,
    cd0,
    ca1,
    cd1,
    stats,
    mixed,
    tokb,
    pbuf,
    stream_s,
    normed,
    outg,
    arr,
    wg,
    wu,
    wd,
    hid,
    outb,
    ret,
    wtab,
    known,
    load_sem,
    halo_send,
    halo_recv,
    stat_sem,
    tok_sem,
    disp_send,
    disp_recv,
    fwd_sem,
    hid_send,
    hid_recv,
    pre_sem,
    ring_send,
    ring_recv,
    ret_send,
    ret_recv,
):
    nz = n_tp // 2
    sp, tp = lax.axis_index("sp"), lax.axis_index("tp")
    z, core = tp // 2, lax.rem(tp, 2)
    other = 1 - core
    sibling = 2 * z + other
    seq, chans = mix_h.shape
    rows, width = resid_h.shape
    half = width // 2
    hs = wg_h.shape[0]
    cap = outg.shape[0] // n_sp
    slots = n_sp * cap
    seg = seq // SEGMENTS

    loads = {}
    drains = []

    def load(src, dst, k):
        copy = pltpu.make_async_copy(src, dst, load_sem.at[k])
        copy.start()
        loads[k] = copy
        return k

    def need(k):
        if k in loads:
            loads.pop(k).wait()

    own_rows = hint(tp * rows, rows)
    l_mix = load(mix_h, mixv, 0)
    l_gate = load(gate_h, gatev, 1)
    l_wg = load(wg_h, wg.at[0], 2)
    l_wu = load(wu_h, wu.at[0], 3)
    l_wd = load(
        wd_h.at[:, pl.ds(hint(core * half, half), half)],
        wd.at[core, 0:hs, :],
        4,
    )
    l_op = load(oproj_h, oproj, 5)
    l_res = load(resid_h, residv, 6)
    pair = pl.ds(hint(z * 2 * rows, 2 * rows), 2 * rows)
    l_rt = load(routes_h.at[:, pair], routv, 7)
    l_wt = load(wts_h.at[:, pair], wtsv, 8)

    barrier = pltpu.get_barrier_semaphore()
    side = 4
    x, y = lax.rem(sp, side), sp // side
    near_by = [(sp, sibling)]
    near_by += [(sp, lax.rem(tp + n_tp + 2 * step, n_tp)) for step in (1, -1)]
    near_by += [(y * side + lax.rem(x + side + step, side), tp) for step in (1, -1)]
    near_by += [(lax.rem(sp + n_sp + side * step, n_sp), tp) for step in (1, -1)]
    partners = near_by + [(lax.rem(sp + n_sp + step, n_sp), tp) for step in (1, -1)]
    for peer in partners:
        pl.semaphore_signal(barrier, inc=1, device_id=peer, device_id_type=MESH)

    heads, hd = rg.shape[1], rg.shape[2]
    wcat[...] = jnp.zeros_like(wcat)
    for d in range(2):
        for which, ref in enumerate((rg, ig)):
            for h in range(heads):
                at = (2 * d + which) * chans + h * hd
                wcat[h * hd : (h + 1) * hd, at : at + hd] = ref[d, h]

    need(l_mix)

    xpad[0:8, :] = jnp.zeros((8, chans), F32)
    xpad[8 : 8 + seq, :] = mixv[...].astype(F32)
    xpad[8 + seq : 16 + seq, :] = jnp.zeros((8, chans), F32)

    def strided(t):
        return xpad[pl.ds(t, SEGMENTS, stride=seg), :]

    taps = [jnp.broadcast_to(conv_w[j : j + 1, :], (SEGMENTS, chans)) for j in range(4)]
    bias = jnp.broadcast_to(conv_b[0:1, :], (SEGMENTS, chans))

    def weigh(x0, x1, x2, x3):
        return bias + x0 * taps[0] + x1 * taps[1] + x2 * taps[2] + x3 * taps[3]

    def conv_body(t, window):
        x0, x1, x2 = window
        x3 = strided(9 + t)
        conv_s[pl.ds(hint(t * SEGMENTS, SEGMENTS), SEGMENTS), :] = weigh(x0, x1, x2, x3)
        return x1, x2, x3

    lax.fori_loop(0, seg, conv_body, (strided(6), strided(7), strided(8)), unroll=8)

    pl.semaphore_wait(barrier, len(partners))

    def tell(k):
        for peer in near_by:
            pl.semaphore_signal(known.at[k], inc=1, device_id=peer, device_id_type=MESH)

    def hear(k):
        pl.semaphore_wait(known.at[k], len(near_by))

    tell(0)

    right = 2 * lax.rem(z + 1, nz) + core
    left = 2 * lax.rem(z + nz - 1, nz) + core

    far, near = nz // 2, nz - 1 - nz // 2
    place = places(nz)

    def hops(direction, piece):
        return far if piece % 2 == direction else near

    def piece_ref(direction, piece, hop):
        at = place[hop if direction == 1 or hop == 0 else nz - hop]
        if piece < 2:
            return (wg, wu)[piece].at[at]
        q = piece - 2
        return wd.at[:, at * hs : (at + 1) * hs, STARTS[q] : STARTS[q] + WIDTHS[q]]

    def ring_copy(direction, piece, hop):
        src = piece_ref(direction, piece, hop - 1)
        if hop == 1 and piece < 2:
            src = (wg_h, wu_h)[piece]
        return pltpu.make_async_remote_copy(
            src_ref=src,
            dst_ref=piece_ref(direction, piece, hop),
            send_sem=ring_send.at[direction, piece, hop - 1],
            recv_sem=ring_recv.at[direction, piece, hop - 1],
            device_id=(sp, right if direction == 0 else left),
            device_id_type=MESH,
        )

    sent = []
    taken = set()
    stage = [0]

    def take(direction, piece, hop):
        if (direction, piece, hop) not in taken:
            taken.add((direction, piece, hop))
            blocked_all(
                piece_ref(direction, piece, hop), ring_recv.at[direction, piece, hop - 1]
            )

    def poll():
        for direction, piece, hop in PLAN[stage[0]]:
            if hop > 1:
                take(direction, piece, hop - 1)
            elif piece >= 2 and "pre" not in taken:
                taken.add("pre")
                need(l_wd)
                pre.wait()
            ring_copy(direction, piece, hop).start()
            sent.append((direction, piece, hop))
        stage[0] += 1

    def complete(piece, end=NEVER):
        for direction in (0, 1):
            for hop in range(1, hops(direction, piece) + 1):
                if place[hop if direction == 1 else nz - hop] < end:
                    assert (direction, piece, hop) in sent
                    take(direction, piece, hop)

    def finish():
        for drain in drains:
            drain()
        for event in sent:
            ring_copy(*event).wait_send()

    nxt, prv = lax.rem(sp + 1, n_sp), lax.rem(sp + n_sp - 1, n_sp)
    hr = halo.shape[1]
    to_next = pltpu.make_async_remote_copy(
        src_ref=mixv.at[seq - hr : seq, :],
        dst_ref=halo.at[0],
        send_sem=halo_send.at[0],
        recv_sem=halo_recv.at[0],
        device_id=(nxt, tp),
        device_id_type=MESH,
    )
    to_prev = pltpu.make_async_remote_copy(
        src_ref=mixv.at[0:hr, :],
        dst_ref=halo.at[1],
        send_sem=halo_send.at[1],
        recv_sem=halo_recv.at[1],
        device_id=(prv, tp),
        device_id_type=MESH,
    )
    to_next.start()
    to_prev.start()

    pre = pltpu.make_async_remote_copy(
        src_ref=wd_h.at[:, pl.ds(hint(other * half, half), half)],
        dst_ref=wd.at[core, 0:hs, :],
        send_sem=pre_sem.at[0],
        recv_sem=pre_sem.at[1],
        device_id=(sp, sibling),
        device_id_type=MESH,
    )
    poll()
    pre.start()

    rates = []
    for d in range(2):
        x = -decay[d : d + 1, :]
        rates.append(-8.0 * (jnp.maximum(x, 0.0) + jnp.log1p(jnp.exp(-jnp.abs(x)))))
    part = 128

    def coefficients(c):
        pre_act = jnp.dot(c, wcat[...], precision=HIGHEST_MODE, preferred_element_type=F32)
        found = []
        for d in range(2):
            r = jax.nn.sigmoid(pre_act[:, 2 * d * chans : (2 * d + 1) * chans] + rb[d : d + 1, :])
            i = jax.nn.sigmoid(
                pre_act[:, (2 * d + 1) * chans : (2 * d + 2) * chans] + ib[d : d + 1, :]
            )
            la = r * rates[d]
            a = jnp.exp(la)
            x = 2.0 * la
            series = 1.0 + x * (1.0 / 6.0)
            for k in (5.0, 4.0, 3.0, 2.0):
                series = 1.0 + x * (1.0 / k) * series
            gap = jnp.where(x > -0.3, -x * series, 1.0 - a * a)
            found += [a, jnp.sqrt(gap) * (i * c)]
        return found

    kept = (ca0, cd0, ca1, cd1)

    def coef_body(n, _):
        at = pl.ds(hint(n * part, part), part)
        for ref, value in zip(kept, coefficients(conv_s[at, :])):
            ref[at, :] = value
        return 0

    lax.fori_loop(0, seq // part // 2, coef_body, 0)
    hear(0)
    tell(1)
    poll()
    lax.fori_loop(seq // part // 2, seq // part, coef_body, 0)
    hear(1)
    tell(2)

    poll()
    to_next.wait()
    to_prev.wait()
    before = jnp.where(sp > 0, 1.0, 0.0).astype(F32)
    after = jnp.where(sp < n_sp - 1, 1.0, 0.0).astype(F32)
    xpad[0:8, :] = halo[0].astype(F32)[hr - 8 : hr] * before
    xpad[8 + seq : 16 + seq, :] = halo[1].astype(F32)[0:8] * after
    ends = jnp.concatenate(
        [weigh(*(strided(6 + t + j) for j in range(4))) for t in (0, 1, seg - 1)], axis=0
    )
    for ref, value in zip(kept, coefficients(ends)):
        ref[0 : 2 * SEGMENTS, :] = value[0 : 2 * SEGMENTS]
        ref[seq - SEGMENTS : seq, :] = value[2 * SEGMENTS :]

    zero = jnp.zeros((SEGMENTS, chans), F32)
    one = jnp.ones((SEGMENTS, chans), F32)

    def scan_body(t, carry):
        f, p, g, q = carry
        fat = pl.ds(hint(t * SEGMENTS, SEGMENTS), SEGMENTS)
        bat = pl.ds(hint((seg - 1 - t) * SEGMENTS, SEGMENTS), SEGMENTS)
        a, b = ca0[fat, :], ca1[bat, :]
        f = a * f + cd0[fat, :]
        p = a * p
        g = b * g + cd1[bat, :]
        q = b * q
        cd0[fat, :] = f
        ca0[fat, :] = p
        cd1[bat, :] = g
        ca1[bat, :] = q
        return f, p, g, q

    f_end, p_end, g_end, q_end = lax.fori_loop(0, seg, scan_body, (zero, one, zero, one), unroll=8)

    poll()
    hear(2)
    tell(3)

    row = lambda v, k: v[k : k + 1, :]
    f_scale, f_shift = [row(one, 0)], [row(zero, 0)]
    for k in range(SEGMENTS):
        f_scale.append(row(p_end, k) * f_scale[-1])
        f_shift.append(row(p_end, k) * f_shift[-1] + row(f_end, k))
    b_scale, b_shift = [row(one, 0)], [row(zero, 0)]
    for k in range(SEGMENTS - 1, -1, -1):
        b_scale.append(row(q_end, k) * b_scale[-1])
        b_shift.append(row(q_end, k) * b_shift[-1] + row(g_end, k))
    for k, v in enumerate((f_scale[-1], f_shift[-1], b_scale[-1], b_shift[-1])):
        stats[sp, k : k + 1, :] = v
    for i in range(1, n_sp):
        pltpu.make_async_remote_copy(
            src_ref=stats.at[sp],
            dst_ref=stats.at[sp],
            send_sem=stat_sem.at[0],
            recv_sem=stat_sem.at[1],
            device_id=(lax.rem(sp + i, n_sp), tp),
            device_id_type=MESH,
        ).start()
    drains.append(lambda: blocked_all(stats.at[0 : n_sp - 1], stat_sem.at[0]))
    poll()

    need(l_gate)

    def gelu_body(n, _):
        at = pl.ds(hint(n * 64, 64), 64)
        xpad[at, :] = jax.nn.gelu(gatev[at, :].astype(F32))
        return 0

    lax.fori_loop(0, seq // 64, gelu_body, 0)
    poll()
    blocked_all(stats.at[0 : n_sp - 1], stat_sem.at[1])

    f_in = jnp.zeros((1, chans), F32)
    b_in = jnp.zeros((1, chans), F32)
    for j in range(n_sp):
        f_in = jnp.where(j < sp, stats[j, 0:1, :] * f_in + stats[j, 1:2, :], f_in)
        k = n_sp - 1 - j
        b_in = jnp.where(k > sp, stats[k, 2:3, :] * b_in + stats[k, 3:4, :], b_in)
    f_enter = jnp.concatenate(
        [f_scale[k] * f_in + f_shift[k] for k in range(SEGMENTS)], axis=0
    )
    b_enter = jnp.concatenate(
        [b_scale[SEGMENTS - 1 - k] * b_in + b_shift[SEGMENTS - 1 - k] for k in range(SEGMENTS)],
        axis=0,
    )

    def join_body(t, _):
        at = pl.ds(hint(t * SEGMENTS, SEGMENTS), SEGMENTS)
        back = pl.ds(t, SEGMENTS, stride=seg)
        state = (cd0[at, :] + ca0[at, :] * f_enter) + (cd1[at, :] + ca1[at, :] * b_enter)
        conv_s[back, :] = state
        return 0

    lax.fori_loop(0, seg, join_body, 0, unroll=8)

    def mix_body(n, _):
        at = pl.ds(hint(n * rows, rows), rows)
        mixed[at, :] = (conv_s[at, :] * xpad[at, :]).astype(BF16)
        return 0

    lax.fori_loop(0, seq // rows, mix_body, 0)
    poll()

    hear(3)
    own_cols = pl.ds(hint(tp * chans, chans), chans)
    for i in range(1, n_tp):
        peer = lax.rem(tp + i, n_tp)
        pltpu.make_async_remote_copy(
            src_ref=mixed.at[pl.ds(hint(peer * rows, rows), rows), :],
            dst_ref=tokb.at[:, own_cols],
            send_sem=tok_sem.at[0],
            recv_sem=tok_sem.at[1],
            device_id=(sp, peer),
            device_id_type=MESH,
        ).start()
    drains.append(lambda: blocked_all(tokb.at[:, 0 : (n_tp - 1) * chans], tok_sem.at[0]))
    tokb[:, own_cols] = mixed[pl.ds(own_rows, rows), :]
    poll()

    need(l_rt)
    need(l_wt)
    lane = lax.broadcasted_iota(jnp.int32, (n_sp, rows), 0)
    own_routes = jnp.where(core == 0, routv[:, 0:rows], routv[:, rows : 2 * rows])
    own_wts = jnp.where(core == 0, wtsv[:, 0:rows], wtsv[:, rows : 2 * rows])
    e0 = jnp.broadcast_to(own_routes[0:1, :], (n_sp, rows))
    e1 = jnp.broadcast_to(own_routes[1:2, :], (n_sp, rows))
    h0 = jnp.where(e0 == lane, 1.0, 0.0)
    h1 = jnp.where(e1 == lane, 1.0, 0.0)
    earlier = jnp.where(
        lax.broadcasted_iota(jnp.int32, (rows, rows), 0)
        < lax.broadcasted_iota(jnp.int32, (rows, rows), 1),
        1.0,
        0.0,
    )
    counts = jnp.dot(
        (h0 + h1).astype(BF16), earlier.astype(BF16), preferred_element_type=F32
    )
    slot0 = jnp.sum(counts * h0, axis=0, keepdims=True).astype(jnp.int32) + own_routes[
        0:1, :
    ] * cap
    slot1 = jnp.sum(counts * h1, axis=0, keepdims=True).astype(jnp.int32) + own_routes[
        1:2, :
    ] * cap
    slot_id = lax.broadcasted_iota(jnp.int32, (slots, rows), 0)
    hit0, hit1 = slot_id == slot0, slot_id == slot1
    sel = jnp.where(hit0 | hit1, 1.0, 0.0).astype(BF16)
    weights = jnp.where(hit0, own_wts[0:1, :], 0.0) + jnp.where(hit1, own_wts[1:2, :], 0.0)
    eye = jnp.where(
        lax.broadcasted_iota(jnp.int32, (rows, rows), 0)
        == lax.broadcasted_iota(jnp.int32, (rows, rows), 1),
        1.0,
        0.0,
    )
    table = lax.dot_general(
        eye,
        weights,
        (((1,), (1,)), ((), ())),
        precision=HIGHEST_MODE,
        preferred_element_type=F32,
    )
    high = table.astype(BF16)
    wtab[0] = high
    wtab[1] = (table - high.astype(F32)).astype(BF16)

    need(l_op)
    need(l_res)
    poll()
    blocked_all(tokb.at[:, 0 : (n_tp - 1) * chans], tok_sem.at[1])
    poll()
    pw = min(512, width)

    def proj_body(n, _):
        at = pl.ds(hint(n * pw, pw), pw)
        pbuf[:, at] = (
            jnp.dot(tokb[...], oproj[:, at], preferred_element_type=F32).astype(BF16).astype(F32)
        )
        return 0

    lax.fori_loop(0, width // pw, proj_body, 0)
    poll()

    def norm_body(n, _):
        at = pl.ds(hint(n * 16, 16), 16)
        v = pbuf[at, :]
        s = (residv[at, :].astype(F32) + v * root_mean(v) * gain[0:1, :]).astype(BF16).astype(F32)
        stream_s[at, :] = s
        normed[at, :] = (s * root_mean(s) * gain[1:2, :]).astype(BF16)
        return 0

    lax.fori_loop(0, rows // 16, norm_body, 0)
    poll()

    gw = min(256, width)

    def dispatch_body(n, _):
        at = pl.ds(hint(n * gw, gw), gw)
        outg[:, at] = jnp.dot(sel, normed[:, at], preferred_element_type=F32).astype(BF16)
        return 0

    lax.fori_loop(0, width // gw, dispatch_body, 0)
    poll()
    own_slots = pl.ds(hint(sp * cap, cap), cap)
    for i in range(1, n_sp):
        peer = lax.rem(sp + i, n_sp)
        pltpu.make_async_remote_copy(
            src_ref=outg.at[pl.ds(hint(peer * cap, cap), cap), :],
            dst_ref=arr.at[core, own_slots, :],
            send_sem=disp_send.at[0],
            recv_sem=disp_recv.at[i - 1],
            device_id=(peer, tp),
            device_id_type=MESH,
        ).start()

    drains.append(lambda: blocked_all(outg.at[0 : slots - cap, :], disp_send.at[0]))

    def forward(src_ref, at):
        pltpu.make_async_remote_copy(
            src_ref=src_ref,
            dst_ref=arr.at[core, at, :],
            send_sem=fwd_sem.at[0],
            recv_sem=fwd_sem.at[1],
            device_id=(sp, sibling),
            device_id_type=MESH,
        ).start()

    forward(outg.at[own_slots, :], own_slots)
    drains.append(lambda: blocked_all(outg, fwd_sem.at[0]))
    arr[core, own_slots, :] = outg[own_slots, :]
    poll()
    for i in range(1, n_sp):
        src = lax.rem(sp + n_sp - i, n_sp)
        at = pl.ds(hint(src * cap, cap), cap)
        blocked_all(arr.at[core, at, :], disp_recv.at[i - 1])
        forward(arr.at[core, at, :], at)
        poll()

    hidden_all = nz * hs
    hw = min(256, hidden_all)
    zh = hw // hs
    dims = (((1,), (1,)), ((), ()))

    def swap(c, k):
        at = hid.at[core, pl.ds(hint(c * slots, slots), slots), k * hw : (k + 1) * hw]
        return pltpu.make_async_remote_copy(
            src_ref=at,
            dst_ref=at,
            send_sem=hid_send.at[c, k],
            recv_sem=hid_recv.at[c, k],
            device_id=(sp, sibling),
            device_id_type=MESH,
        )

    def gate_block(c, k):
        x = arr[c]
        g, u = (
            lax.dot_general(
                x,
                w[k * zh : (k + 1) * zh].reshape(hw, width),
                dims,
                preferred_element_type=F32,
            )
            for w in (wg, wu)
        )
        hid[core, pl.ds(hint(c * slots, slots), slots), k * hw : (k + 1) * hw] = (
            g * jax.nn.sigmoid(g) * u
        ).astype(BF16)
        swap(c, k).start()
        drains.append(swap(c, k).wait_send)
        poll()

    need(l_wg)
    need(l_wu)
    blocks = hidden_all // hw
    for k in range(blocks):
        last = k == blocks - 1
        if last:
            poll()
        complete(0, zh * (k + 1))
        complete(1, zh * (k + 1))
        if last:
            poll()
        gate_block(core, k)
        if k == 0:
            blocked_all(arr.at[other], fwd_sem.at[1])
        gate_block(other, k)
    poll()
    for k in range(blocks):
        for c in range(2):
            swap(c, k).wait_recv()

    for q in range(CHUNKS):
        cols = slice(STARTS[q], STARTS[q] + WIDTHS[q])
        poll()
        poll()
        complete(2 + q)
        poll()

        hm = min(256, slots)

        def down_body(n, _):
            at = pl.ds(hint(n * hm, hm), hm)
            o = jnp.dot(
                hid[0, at, :], wd[0, :, cols], preferred_element_type=F32
            ) + jnp.dot(hid[1, at, :], wd[1, :, cols], preferred_element_type=F32)
            outb[q][at, :] = o.astype(BF16)
            return 0

        lax.fori_loop(0, 2 * slots // hm, down_body, 0)
        poll()
        for i in range(n_sp):
            peer = lax.rem(sp + i, n_sp)
            for mine in (1, 0):
                if i == 0 and mine:
                    continue
                c = core if mine else other
                pltpu.make_async_remote_copy(
                    src_ref=outb[q].at[pl.ds(hint(c * slots + peer * cap, cap), cap), :],
                    dst_ref=ret[q].at[core, own_slots, :],
                    send_sem=ret_send.at[q, mine],
                    recv_sem=ret_recv.at[q, mine],
                    device_id=(peer, tp if mine else sibling),
                    device_id_type=MESH,
                ).start()
        drains.append(
            lambda q=q: blocked_all(ret[q].at[core, 0 : slots - cap, :], ret_send.at[q, 1])
        )
        drains.append(lambda q=q: blocked_all(ret[q].at[other], ret_send.at[q, 0]))
        ret[q][core, own_slots, :] = outb[q][
            pl.ds(hint(core * slots + sp * cap, cap), cap), :
        ]
        poll()

    for q in range(CHUNKS):
        blocked_all(ret[q].at[core, 0 : slots - cap, :], ret_recv.at[q, 1])
        blocked_all(ret[q].at[other], ret_recv.at[q, 0])
        for c in range(2):
            v = ret[q][c]
            o = jnp.dot(wtab[0], v, preferred_element_type=F32) + jnp.dot(
                wtab[1], v, preferred_element_type=F32
            )
            at = c * half + STARTS[q]
            pbuf[:, at : at + WIDTHS[q]] = o.astype(BF16).astype(F32)

    def final_body(n, _):
        at = pl.ds(hint(n * 16, 16), 16)
        v = pbuf[at, :]
        out_ref[at, :] = (stream_s[at, :] + v * root_mean(v) * gain[2:3, :]).astype(BF16)
        return 0

    lax.fori_loop(0, rows // 16, final_body, 0)

    finish()


def on_device(
    mix_in,
    gate_in,
    conv_w,
    conv_b,
    decay_param,
    recur_gate,
    recur_bias,
    input_gate,
    input_bias,
    residual,
    out_proj,
    norm_gain,
    routes,
    route_wt,
    exp_gate,
    exp_up,
    exp_down,
):
    n_sp, n_tp = lax.axis_size("sp"), lax.axis_size("tp")
    nz = n_tp // 2
    seq, chans = mix_in.shape
    rows, width = residual.shape
    top = routes.shape[1]
    experts = n_sp * exp_gate.shape[0]
    cap = 2 * rows * top // experts
    slots = experts * cap
    hs = exp_gate.shape[2]
    half = width // 2
    far = nz // 2
    pieces = 2 + CHUNKS

    anywhere = pl.BlockSpec(memory_space=pltpu.HBM)
    onchip = pl.BlockSpec(memory_space=pltpu.VMEM)
    dma = pltpu.SemaphoreType.DMA
    scratch = [
        pltpu.VMEM((seq, chans), BF16),
        pltpu.VMEM((seq, chans), BF16),
        pltpu.VMEM((rows, width), BF16),
        pltpu.VMEM(out_proj.shape, BF16),
        pltpu.VMEM((top, 2 * rows), jnp.int32),
        pltpu.VMEM((top, 2 * rows), F32),
        pltpu.VMEM((2, 16, chans), BF16),
        pltpu.VMEM((seq + 16, chans), F32),
        pltpu.VMEM((seq, chans), F32),
        pltpu.VMEM((chans, 4 * chans), F32),
        pltpu.VMEM((seq, chans), F32),
        pltpu.VMEM((seq, chans), F32),
        pltpu.VMEM((seq, chans), F32),
        pltpu.VMEM((seq, chans), F32),
        pltpu.VMEM((n_sp, 8, chans), F32),
        pltpu.VMEM((seq, chans), BF16),
        pltpu.VMEM((rows, n_tp * chans), BF16),
        pltpu.VMEM((rows, width), F32),
        pltpu.VMEM((rows, width), F32),
        pltpu.VMEM((rows, width), BF16),
        pltpu.VMEM((slots, width), BF16),
        pltpu.VMEM((2, slots, width), BF16),
        pltpu.VMEM((nz, hs, width), BF16),
        pltpu.VMEM((nz, hs, width), BF16),
        pltpu.VMEM((2, nz * hs, half), BF16),
        pltpu.VMEM((2, 2 * slots, nz * hs), BF16),
        [pltpu.VMEM((2 * slots, w), BF16) for w in WIDTHS],
        [pltpu.VMEM((2, slots, w), BF16) for w in WIDTHS],
        pltpu.VMEM((2, rows, slots), BF16),
        pltpu.SemaphoreType.REGULAR((4,)),
        dma((9,)),
        dma((2,)),
        dma((2,)),
        dma((2,)),
        dma((2,)),
        dma((1,)),
        dma((n_sp - 1,)),
        dma((2,)),
        dma((2, nz * hs // min(256, nz * hs))),
        dma((2, nz * hs // min(256, nz * hs))),
        dma((2,)),
        dma((2, pieces, far)),
        dma((2, pieces, far)),
        dma((CHUNKS, 2)),
        dma((CHUNKS, 2)),
    ]
    where = [
        anywhere,
        anywhere,
        onchip,
        onchip,
        onchip,
        onchip,
        onchip,
        onchip,
        onchip,
        anywhere,
        anywhere,
        onchip,
        anywhere,
        anywhere,
        anywhere,
        anywhere,
        anywhere,
    ]
    return pl.pallas_call(
        functools.partial(kernel, n_sp, n_tp),
        out_shape=jax.ShapeDtypeStruct((rows, width), BF16),
        in_specs=where,
        out_specs=onchip,
        scratch_shapes=scratch,
        compiler_params=pltpu.CompilerParams(
            collective_id=0, has_side_effects=True, vmem_limit_bytes=60 * 1024 * 1024
        ),
    )(
        mix_in,
        gate_in,
        conv_w,
        conv_b.reshape(1, chans),
        decay_param,
        recur_gate,
        recur_bias,
        input_gate,
        input_bias,
        residual,
        out_proj,
        norm_gain,
        routes.T,
        route_wt.T,
        exp_gate[0].T,
        exp_up[0].T,
        exp_down[0],
    )


def solution(mesh):
    return jax.shard_map(
        on_device,
        mesh=mesh,
        in_specs=(
            P("sp", "tp"),
            P("sp", "tp"),
            P(None, "tp"),
            P("tp"),
            P(None, "tp"),
            P(None, "tp", None, None),
            P(None, "tp"),
            P(None, "tp", None, None),
            P(None, "tp"),
            P(("sp", "tp"), None),
            P(),
            P(),
            P("sp", None),
            P("sp", None),
            P("sp", None, "tp"),
            P("sp", None, "tp"),
            P("sp", "tp", None),
        ),
        out_specs=P(("sp", "tp"), None),
        check_vma=False,
    )
```

```python
import functools

import jax
import jax.numpy as jnp
from jax import lax
from jax.experimental import pallas as pl
from jax.experimental.pallas import tpu as pltpu
from jax.sharding import PartitionSpec as P

EPSILON = 1e-06
HIGHEST_MODE = lax.Precision.HIGHEST
MESH = pl.DeviceIdType.MESH
F32, BF16 = jnp.float32, jnp.bfloat16
SEGMENTS = 8
WIDTHS = (128, 128, 128, 128, 256, 256)
CHUNKS = len(WIDTHS)
NEVER = 1 << 20
PLAN = (
    ((0, 0, 1), (0, 1, 1), (1, 1, 1), (1, 0, 1),),
    (),
    ((0, 2, 1), (0, 3, 1), (0, 4, 1), (0, 5, 1), (1, 2, 1), (1, 3, 1), (1, 4, 1), (1, 5, 1),),
    (),
    (),
    (),
    ((0, 0, 2), (1, 1, 2),),
    (),
    ((0, 1, 2), (1, 0, 2), (0, 4, 2), (0, 5, 2), (0, 2, 2), (0, 3, 2), (0, 0, 3), (1, 4, 2), (1, 5, 2), (1, 2, 2), (1, 3, 2), (1, 1, 3),),
    (),
    (),
    (),
    (),
    (),
    ((0, 6, 1), (1, 6, 1), (0, 1, 3), (1, 7, 1), (1, 0, 3),),
    (),
    (),
    (),
    ((0, 2, 3),),
    ((0, 3, 3),),
    ((1, 2, 3),),
    ((1, 3, 3),),
    (),
    ((0, 0, 4), (1, 1, 4),),
    (),
    (),
    (),
    (),
    (),
    (),
    ((0, 6, 2), (0, 7, 1), (0, 4, 3), (0, 5, 3), (1, 6, 2), (1, 7, 2), (1, 4, 3),),
    (),
    ((0, 2, 4), (1, 5, 3), (1, 3, 4),),
    ((0, 6, 3),),
    (),
    ((0, 7, 2), (1, 6, 3), (0, 4, 4),),
    (),
    (),
    ((1, 7, 3),),
    (),
    ((1, 5, 4),),
    (),
    (),
    (),
    (),
    ((0, 6, 4),),
    (),
    (),
    ((0, 7, 3),),
    (),
    (),
    (),
    (),
    ((1, 7, 4),),
    (),
    (),
    (),
    (),
    (),
    (),
    (),
    (),
    (),
    (),
    (),
    (),
)
STARTS = tuple(sum(WIDTHS[:k]) for k in range(CHUNKS))


def hint(value, step):
    return pl.multiple_of(value, step)


def blocked_all(copy_ref, sem):
    pltpu.make_async_copy(copy_ref, copy_ref, sem).wait()


def root_mean(values):
    return lax.rsqrt(jnp.mean(values * values, axis=-1, keepdims=True) + EPSILON)


def places(nz):
    order = [0]
    for step in range(1, nz // 2 + 1):
        order += [step, nz - step] if step < nz - step else [step]
    return {distance: place for place, distance in enumerate(order)}


def kernel(
    n_sp,
    n_tp,
    mix_h,
    gate_h,
    conv_w,
    conv_b,
    decay,
    rg,
    rb,
    ig,
    ib,
    resid_h,
    oproj_h,
    gain,
    routes_h,
    wts_h,
    wg_h,
    wu_h,
    wd_h,
    out_ref,
    mixv,
    gatev,
    residv,
    oproj,
    routv,
    wtsv,
    halo,
    xpad,
    conv_s,
    wcat,
    ca0,
    cd0,
    ca1,
    cd1,
    stats,
    mixed,
    tokb,
    pbuf,
    stream_s,
    normed,
    outg,
    arr,
    wg,
    wu,
    wd,
    hid,
    outb,
    ret,
    wtab,
    known,
    load_sem,
    halo_send,
    halo_recv,
    stat_sem,
    tok_sem,
    disp_send,
    disp_recv,
    fwd_sem,
    hid_send,
    hid_recv,
    pre_sem,
    ring_send,
    ring_recv,
    ret_send,
    ret_recv,
):
    nz = n_tp // 2
    sp, tp = lax.axis_index("sp"), lax.axis_index("tp")
    z, core = tp // 2, lax.rem(tp, 2)
    other = 1 - core
    sibling = 2 * z + other
    seq, chans = mix_h.shape
    rows, width = resid_h.shape
    half = width // 2
    hs = wg_h.shape[0]
    cap = outg.shape[0] // n_sp
    slots = n_sp * cap
    seg = seq // SEGMENTS

    loads = {}
    drains = []

    def load(src, dst, k):
        copy = pltpu.make_async_copy(src, dst, load_sem.at[k])
        copy.start()
        loads[k] = copy
        return k

    def need(k):
        if k in loads:
            loads.pop(k).wait()

    own_rows = hint(tp * rows, rows)
    l_mix = load(mix_h, mixv, 0)
    l_gate = load(gate_h, gatev, 1)
    l_wg = load(wg_h, wg.at[0], 2)
    l_wu = load(wu_h, wu.at[0], 3)
    l_wd = load(
        wd_h.at[:, pl.ds(hint(core * half, half), half)],
        wd.at[core, 0:hs, :],
        4,
    )
    l_op = load(oproj_h, oproj, 5)
    l_res = load(resid_h, residv, 6)
    pair = pl.ds(hint(z * 2 * rows, 2 * rows), 2 * rows)
    l_rt = load(routes_h.at[:, pair], routv, 7)
    l_wt = load(wts_h.at[:, pair], wtsv, 8)

    barrier = pltpu.get_barrier_semaphore()
    side = 4
    x, y = lax.rem(sp, side), sp // side
    near_by = [(sp, sibling)]
    near_by += [(sp, lax.rem(tp + n_tp + 2 * step, n_tp)) for step in (1, -1)]
    near_by += [(y * side + lax.rem(x + side + step, side), tp) for step in (1, -1)]
    near_by += [(lax.rem(sp + n_sp + side * step, n_sp), tp) for step in (1, -1)]
    partners = near_by + [(lax.rem(sp + n_sp + step, n_sp), tp) for step in (1, -1)]
    for peer in partners:
        pl.semaphore_signal(barrier, inc=1, device_id=peer, device_id_type=MESH)

    heads, hd = rg.shape[1], rg.shape[2]
    wcat[...] = jnp.zeros_like(wcat)
    for d in range(2):
        for which, ref in enumerate((rg, ig)):
            for h in range(heads):
                at = (2 * d + which) * chans + h * hd
                wcat[h * hd : (h + 1) * hd, at : at + hd] = ref[d, h]

    need(l_mix)

    xpad[0:8, :] = jnp.zeros((8, chans), F32)
    xpad[8 : 8 + seq, :] = mixv[...].astype(F32)
    xpad[8 + seq : 16 + seq, :] = jnp.zeros((8, chans), F32)

    def strided(t):
        return xpad[pl.ds(t, SEGMENTS, stride=seg), :]

    taps = [jnp.broadcast_to(conv_w[j : j + 1, :], (SEGMENTS, chans)) for j in range(4)]
    bias = jnp.broadcast_to(conv_b[0:1, :], (SEGMENTS, chans))

    def weigh(x0, x1, x2, x3):
        return bias + x0 * taps[0] + x1 * taps[1] + x2 * taps[2] + x3 * taps[3]

    def conv_body(t, window):
        x0, x1, x2 = window
        x3 = strided(9 + t)
        conv_s[pl.ds(hint(t * SEGMENTS, SEGMENTS), SEGMENTS), :] = weigh(x0, x1, x2, x3)
        return x1, x2, x3

    lax.fori_loop(0, seg, conv_body, (strided(6), strided(7), strided(8)), unroll=8)

    pl.semaphore_wait(barrier, len(partners))

    def tell(k):
        for peer in near_by:
            pl.semaphore_signal(known.at[k], inc=1, device_id=peer, device_id_type=MESH)

    def hear(k):
        pl.semaphore_wait(known.at[k], len(near_by))

    tell(0)

    right = 2 * lax.rem(z + 1, nz) + core
    left = 2 * lax.rem(z + nz - 1, nz) + core

    far, near = nz // 2, nz - 1 - nz // 2
    place = places(nz)

    def hops(direction, piece):
        return far if piece % 2 == direction else near

    def piece_ref(direction, piece, hop):
        at = place[hop if direction == 1 or hop == 0 else nz - hop]
        if piece < 2:
            return (wg, wu)[piece].at[at]
        q = piece - 2
        return wd.at[:, at * hs : (at + 1) * hs, STARTS[q] : STARTS[q] + WIDTHS[q]]

    def ring_copy(direction, piece, hop):
        src = piece_ref(direction, piece, hop - 1)
        if hop == 1 and piece < 2:
            src = (wg_h, wu_h)[piece]
        return pltpu.make_async_remote_copy(
            src_ref=src,
            dst_ref=piece_ref(direction, piece, hop),
            send_sem=ring_send.at[direction, piece, hop - 1],
            recv_sem=ring_recv.at[direction, piece, hop - 1],
            device_id=(sp, right if direction == 0 else left),
            device_id_type=MESH,
        )

    sent = []
    taken = set()
    stage = [0]

    def take(direction, piece, hop):
        if (direction, piece, hop) not in taken:
            taken.add((direction, piece, hop))
            blocked_all(
                piece_ref(direction, piece, hop), ring_recv.at[direction, piece, hop - 1]
            )

    def poll():
        for direction, piece, hop in PLAN[stage[0]]:
            if hop > 1:
                take(direction, piece, hop - 1)
            elif piece >= 2 and "pre" not in taken:
                taken.add("pre")
                need(l_wd)
                pre.wait()
            ring_copy(direction, piece, hop).start()
            sent.append((direction, piece, hop))
        stage[0] += 1

    def complete(piece, end=NEVER):
        for direction in (0, 1):
            for hop in range(1, hops(direction, piece) + 1):
                if place[hop if direction == 1 else nz - hop] < end:
                    assert (direction, piece, hop) in sent
                    take(direction, piece, hop)

    def finish():
        for drain in drains:
            drain()
        for event in sent:
            ring_copy(*event).wait_send()

    nxt, prv = lax.rem(sp + 1, n_sp), lax.rem(sp + n_sp - 1, n_sp)
    hr = halo.shape[1]
    to_next = pltpu.make_async_remote_copy(
        src_ref=mixv.at[seq - hr : seq, :],
        dst_ref=halo.at[0],
        send_sem=halo_send.at[0],
        recv_sem=halo_recv.at[0],
        device_id=(nxt, tp),
        device_id_type=MESH,
    )
    to_prev = pltpu.make_async_remote_copy(
        src_ref=mixv.at[0:hr, :],
        dst_ref=halo.at[1],
        send_sem=halo_send.at[1],
        recv_sem=halo_recv.at[1],
        device_id=(prv, tp),
        device_id_type=MESH,
    )
    to_next.start()
    to_prev.start()

    pre = pltpu.make_async_remote_copy(
        src_ref=wd_h.at[:, pl.ds(hint(other * half, half), half)],
        dst_ref=wd.at[core, 0:hs, :],
        send_sem=pre_sem.at[0],
        recv_sem=pre_sem.at[1],
        device_id=(sp, sibling),
        device_id_type=MESH,
    )
    poll()
    pre.start()

    rates = []
    for d in range(2):
        x = -decay[d : d + 1, :]
        rates.append(-8.0 * (jnp.maximum(x, 0.0) + jnp.log1p(jnp.exp(-jnp.abs(x)))))
    part = 128

    def coefficients(c):
        pre_act = jnp.dot(c, wcat[...], precision=HIGHEST_MODE, preferred_element_type=F32)
        found = []
        for d in range(2):
            r = jax.nn.sigmoid(pre_act[:, 2 * d * chans : (2 * d + 1) * chans] + rb[d : d + 1, :])
            i = jax.nn.sigmoid(
                pre_act[:, (2 * d + 1) * chans : (2 * d + 2) * chans] + ib[d : d + 1, :]
            )
            la = r * rates[d]
            a = jnp.exp(la)
            x = 2.0 * la
            series = 1.0 + x * (1.0 / 6.0)
            for k in (5.0, 4.0, 3.0, 2.0):
                series = 1.0 + x * (1.0 / k) * series
            gap = jnp.where(x > -0.3, -x * series, 1.0 - a * a)
            found += [a, jnp.sqrt(gap) * (i * c)]
        return found

    kept = (ca0, cd0, ca1, cd1)

    def coef_body(n, _):
        at = pl.ds(hint(n * part, part), part)
        for ref, value in zip(kept, coefficients(conv_s[at, :])):
            ref[at, :] = value
        return 0

    lax.fori_loop(0, seq // part // 2, coef_body, 0)
    hear(0)
    tell(1)
    poll()
    lax.fori_loop(seq // part // 2, seq // part, coef_body, 0)
    hear(1)
    tell(2)

    poll()
    to_next.wait()
    to_prev.wait()
    before = jnp.where(sp > 0, 1.0, 0.0).astype(F32)
    after = jnp.where(sp < n_sp - 1, 1.0, 0.0).astype(F32)
    xpad[0:8, :] = halo[0].astype(F32)[hr - 8 : hr] * before
    xpad[8 + seq : 16 + seq, :] = halo[1].astype(F32)[0:8] * after
    ends = jnp.concatenate(
        [weigh(*(strided(6 + t + j) for j in range(4))) for t in (0, 1, seg - 1)], axis=0
    )
    for ref, value in zip(kept, coefficients(ends)):
        ref[0 : 2 * SEGMENTS, :] = value[0 : 2 * SEGMENTS]
        ref[seq - SEGMENTS : seq, :] = value[2 * SEGMENTS :]

    zero = jnp.zeros((SEGMENTS, chans), F32)
    one = jnp.ones((SEGMENTS, chans), F32)

    def scan_body(t, carry):
        f, p, g, q = carry
        fat = pl.ds(hint(t * SEGMENTS, SEGMENTS), SEGMENTS)
        bat = pl.ds(hint((seg - 1 - t) * SEGMENTS, SEGMENTS), SEGMENTS)
        a, b = ca0[fat, :], ca1[bat, :]
        f = a * f + cd0[fat, :]
        p = a * p
        g = b * g + cd1[bat, :]
        q = b * q
        cd0[fat, :] = f
        ca0[fat, :] = p
        cd1[bat, :] = g
        ca1[bat, :] = q
        return f, p, g, q

    f_end, p_end, g_end, q_end = lax.fori_loop(0, seg, scan_body, (zero, one, zero, one), unroll=8)

    poll()
    hear(2)
    tell(3)

    row = lambda v, k: v[k : k + 1, :]
    f_scale, f_shift = [row(one, 0)], [row(zero, 0)]
    for k in range(SEGMENTS):
        f_scale.append(row(p_end, k) * f_scale[-1])
        f_shift.append(row(p_end, k) * f_shift[-1] + row(f_end, k))
    b_scale, b_shift = [row(one, 0)], [row(zero, 0)]
    for k in range(SEGMENTS - 1, -1, -1):
        b_scale.append(row(q_end, k) * b_scale[-1])
        b_shift.append(row(q_end, k) * b_shift[-1] + row(g_end, k))
    for k, v in enumerate((f_scale[-1], f_shift[-1], b_scale[-1], b_shift[-1])):
        stats[sp, k : k + 1, :] = v
    for i in range(1, n_sp):
        pltpu.make_async_remote_copy(
            src_ref=stats.at[sp],
            dst_ref=stats.at[sp],
            send_sem=stat_sem.at[0],
            recv_sem=stat_sem.at[1],
            device_id=(lax.rem(sp + i, n_sp), tp),
            device_id_type=MESH,
        ).start()
    drains.append(lambda: blocked_all(stats.at[0 : n_sp - 1], stat_sem.at[0]))
    poll()

    need(l_gate)

    def gelu_body(n, _):
        at = pl.ds(hint(n * 64, 64), 64)
        xpad[at, :] = jax.nn.gelu(gatev[at, :].astype(F32))
        return 0

    lax.fori_loop(0, seq // 64, gelu_body, 0)
    poll()
    blocked_all(stats.at[0 : n_sp - 1], stat_sem.at[1])

    f_in = jnp.zeros((1, chans), F32)
    b_in = jnp.zeros((1, chans), F32)
    for j in range(n_sp):
        f_in = jnp.where(j < sp, stats[j, 0:1, :] * f_in + stats[j, 1:2, :], f_in)
        k = n_sp - 1 - j
        b_in = jnp.where(k > sp, stats[k, 2:3, :] * b_in + stats[k, 3:4, :], b_in)
    f_enter = jnp.concatenate(
        [f_scale[k] * f_in + f_shift[k] for k in range(SEGMENTS)], axis=0
    )
    b_enter = jnp.concatenate(
        [b_scale[SEGMENTS - 1 - k] * b_in + b_shift[SEGMENTS - 1 - k] for k in range(SEGMENTS)],
        axis=0,
    )

    def join_body(t, _):
        at = pl.ds(hint(t * SEGMENTS, SEGMENTS), SEGMENTS)
        back = pl.ds(t, SEGMENTS, stride=seg)
        state = (cd0[at, :] + ca0[at, :] * f_enter) + (cd1[at, :] + ca1[at, :] * b_enter)
        conv_s[back, :] = state
        return 0

    lax.fori_loop(0, seg, join_body, 0, unroll=8)

    def mix_body(n, _):
        at = pl.ds(hint(n * rows, rows), rows)
        mixed[at, :] = (conv_s[at, :] * xpad[at, :]).astype(BF16)
        return 0

    lax.fori_loop(0, seq // rows, mix_body, 0)
    poll()

    hear(3)
    own_cols = pl.ds(hint(tp * chans, chans), chans)
    for i in range(1, n_tp):
        peer = lax.rem(tp + i, n_tp)
        pltpu.make_async_remote_copy(
            src_ref=mixed.at[pl.ds(hint(peer * rows, rows), rows), :],
            dst_ref=tokb.at[:, own_cols],
            send_sem=tok_sem.at[0],
            recv_sem=tok_sem.at[1],
            device_id=(sp, peer),
            device_id_type=MESH,
        ).start()
    drains.append(lambda: blocked_all(tokb.at[:, 0 : (n_tp - 1) * chans], tok_sem.at[0]))
    tokb[:, own_cols] = mixed[pl.ds(own_rows, rows), :]
    poll()

    need(l_rt)
    need(l_wt)
    lane = lax.broadcasted_iota(jnp.int32, (n_sp, rows), 0)
    own_routes = jnp.where(core == 0, routv[:, 0:rows], routv[:, rows : 2 * rows])
    own_wts = jnp.where(core == 0, wtsv[:, 0:rows], wtsv[:, rows : 2 * rows])
    e0 = jnp.broadcast_to(own_routes[0:1, :], (n_sp, rows))
    e1 = jnp.broadcast_to(own_routes[1:2, :], (n_sp, rows))
    h0 = jnp.where(e0 == lane, 1.0, 0.0)
    h1 = jnp.where(e1 == lane, 1.0, 0.0)
    earlier = jnp.where(
        lax.broadcasted_iota(jnp.int32, (rows, rows), 0)
        < lax.broadcasted_iota(jnp.int32, (rows, rows), 1),
        1.0,
        0.0,
    )
    counts = jnp.dot(
        (h0 + h1).astype(BF16), earlier.astype(BF16), preferred_element_type=F32
    )
    slot0 = jnp.sum(counts * h0, axis=0, keepdims=True).astype(jnp.int32) + own_routes[
        0:1, :
    ] * cap
    slot1 = jnp.sum(counts * h1, axis=0, keepdims=True).astype(jnp.int32) + own_routes[
        1:2, :
    ] * cap
    slot_id = lax.broadcasted_iota(jnp.int32, (slots, rows), 0)
    hit0, hit1 = slot_id == slot0, slot_id == slot1
    sel = jnp.where(hit0 | hit1, 1.0, 0.0).astype(BF16)
    weights = jnp.where(hit0, own_wts[0:1, :], 0.0) + jnp.where(hit1, own_wts[1:2, :], 0.0)
    eye = jnp.where(
        lax.broadcasted_iota(jnp.int32, (rows, rows), 0)
        == lax.broadcasted_iota(jnp.int32, (rows, rows), 1),
        1.0,
        0.0,
    )
    table = lax.dot_general(
        eye,
        weights,
        (((1,), (1,)), ((), ())),
        precision=HIGHEST_MODE,
        preferred_element_type=F32,
    )
    high = table.astype(BF16)
    wtab[0:rows, :] = high
    wtab[rows : 2 * rows, :] = (table - high.astype(F32)).astype(BF16)

    need(l_op)
    need(l_res)
    poll()
    blocked_all(tokb.at[:, 0 : (n_tp - 1) * chans], tok_sem.at[1])
    poll()
    pw = min(512, width)

    def proj_body(n, _):
        at = pl.ds(hint(n * pw, pw), pw)
        pbuf[:, at] = (
            jnp.dot(tokb[...], oproj[:, at], preferred_element_type=F32).astype(BF16).astype(F32)
        )
        return 0

    lax.fori_loop(0, width // pw, proj_body, 0)
    poll()

    def norm_body(n, _):
        at = pl.ds(hint(n * 16, 16), 16)
        v = pbuf[at, :]
        s = (residv[at, :].astype(F32) + v * root_mean(v) * gain[0:1, :]).astype(BF16).astype(F32)
        stream_s[at, :] = s
        normed[at, :] = (s * root_mean(s) * gain[1:2, :]).astype(BF16)
        return 0

    lax.fori_loop(0, rows // 16, norm_body, 0)
    poll()

    gw = min(256, width)

    def dispatch_body(n, _):
        at = pl.ds(hint(n * gw, gw), gw)
        outg[:, at] = jnp.dot(sel, normed[:, at], preferred_element_type=F32).astype(BF16)
        return 0

    lax.fori_loop(0, width // gw, dispatch_body, 0)
    poll()
    own_slots = pl.ds(hint(sp * cap, cap), cap)
    for i in range(1, n_sp):
        peer = lax.rem(sp + i, n_sp)
        pltpu.make_async_remote_copy(
            src_ref=outg.at[pl.ds(hint(peer * cap, cap), cap), :],
            dst_ref=arr.at[core, own_slots, :],
            send_sem=disp_send.at[0],
            recv_sem=disp_recv.at[i - 1],
            device_id=(peer, tp),
            device_id_type=MESH,
        ).start()

    drains.append(lambda: blocked_all(outg.at[0 : slots - cap, :], disp_send.at[0]))

    def forward(src_ref, at):
        pltpu.make_async_remote_copy(
            src_ref=src_ref,
            dst_ref=arr.at[core, at, :],
            send_sem=fwd_sem.at[0],
            recv_sem=fwd_sem.at[1],
            device_id=(sp, sibling),
            device_id_type=MESH,
        ).start()

    forward(outg.at[own_slots, :], own_slots)
    drains.append(lambda: blocked_all(outg, fwd_sem.at[0]))
    arr[core, own_slots, :] = outg[own_slots, :]
    poll()
    for i in range(1, n_sp):
        src = lax.rem(sp + n_sp - i, n_sp)
        at = pl.ds(hint(src * cap, cap), cap)
        blocked_all(arr.at[core, at, :], disp_recv.at[i - 1])
        forward(arr.at[core, at, :], at)
        poll()

    hidden_all = nz * hs
    hw = min(256, hidden_all)
    zh = hw // hs
    dims = (((1,), (1,)), ((), ()))

    def swap(c, k):
        at = hid.at[core, pl.ds(hint(c * slots, slots), slots), k * hw : (k + 1) * hw]
        return pltpu.make_async_remote_copy(
            src_ref=at,
            dst_ref=at,
            send_sem=hid_send.at[c, k],
            recv_sem=hid_recv.at[c, k],
            device_id=(sp, sibling),
            device_id_type=MESH,
        )

    def gate_block(c, k):
        x = arr[c]
        g, u = (
            lax.dot_general(
                x,
                w[k * zh : (k + 1) * zh].reshape(hw, width),
                dims,
                preferred_element_type=F32,
            )
            for w in (wg, wu)
        )
        hid[core, pl.ds(hint(c * slots, slots), slots), k * hw : (k + 1) * hw] = (
            g * jax.nn.sigmoid(g) * u
        ).astype(BF16)
        swap(c, k).start()
        drains.append(swap(c, k).wait_send)
        poll()

    need(l_wg)
    need(l_wu)
    blocks = hidden_all // hw
    for k in range(blocks):
        last = k == blocks - 1
        if last:
            poll()
        complete(0, zh * (k + 1))
        complete(1, zh * (k + 1))
        if last:
            poll()
        gate_block(core, k)
        if k == 0:
            blocked_all(arr.at[other], fwd_sem.at[1])
        gate_block(other, k)
    poll()
    for k in range(blocks):
        for c in range(2):
            swap(c, k).wait_recv()

    for q in range(CHUNKS):
        cols = slice(STARTS[q], STARTS[q] + WIDTHS[q])
        poll()
        poll()
        complete(2 + q)
        poll()

        hm = min(256, slots)

        def down_body(n, _):
            at = pl.ds(hint(n * hm, hm), hm)
            o = jnp.dot(
                hid[0, at, :], wd[0, :, cols], preferred_element_type=F32
            ) + jnp.dot(hid[1, at, :], wd[1, :, cols], preferred_element_type=F32)
            outb[q][at, :] = o.astype(BF16)
            return 0

        lax.fori_loop(0, 2 * slots // hm, down_body, 0)
        poll()
        for i in range(n_sp):
            peer = lax.rem(sp + i, n_sp)
            for mine in (1, 0):
                if i == 0 and mine:
                    continue
                c = core if mine else other
                pltpu.make_async_remote_copy(
                    src_ref=outb[q].at[pl.ds(hint(c * slots + peer * cap, cap), cap), :],
                    dst_ref=ret[q].at[core, own_slots, :],
                    send_sem=ret_send.at[q, mine],
                    recv_sem=ret_recv.at[q, mine],
                    device_id=(peer, tp if mine else sibling),
                    device_id_type=MESH,
                ).start()
        drains.append(
            lambda q=q: blocked_all(ret[q].at[core, 0 : slots - cap, :], ret_send.at[q, 1])
        )
        drains.append(lambda q=q: blocked_all(ret[q].at[other], ret_send.at[q, 0]))
        ret[q][core, own_slots, :] = outb[q][
            pl.ds(hint(core * slots + sp * cap, cap), cap), :
        ]
        poll()

    for q in range(CHUNKS):
        blocked_all(ret[q].at[core, 0 : slots - cap, :], ret_recv.at[q, 1])
        blocked_all(ret[q].at[other], ret_recv.at[q, 0])
        for c in range(2):
            v = ret[q][c]
            both = jnp.dot(wtab[...], v, preferred_element_type=F32)
            o = both[0:rows] + both[rows : 2 * rows]
            at = c * half + STARTS[q]
            pbuf[:, at : at + WIDTHS[q]] = o.astype(BF16).astype(F32)

    def final_body(n, _):
        at = pl.ds(hint(n * 16, 16), 16)
        v = pbuf[at, :]
        out_ref[at, :] = (stream_s[at, :] + v * root_mean(v) * gain[2:3, :]).astype(BF16)
        return 0

    lax.fori_loop(0, rows // 16, final_body, 0)

    finish()


def on_device(
    mix_in,
    gate_in,
    conv_w,
    conv_b,
    decay_param,
    recur_gate,
    recur_bias,
    input_gate,
    input_bias,
    residual,
    out_proj,
    norm_gain,
    routes,
    route_wt,
    exp_gate,
    exp_up,
    exp_down,
):
    n_sp, n_tp = lax.axis_size("sp"), lax.axis_size("tp")
    nz = n_tp // 2
    seq, chans = mix_in.shape
    rows, width = residual.shape
    top = routes.shape[1]
    experts = n_sp * exp_gate.shape[0]
    cap = 2 * rows * top // experts
    slots = experts * cap
    hs = exp_gate.shape[2]
    half = width // 2
    far = nz // 2
    pieces = 2 + CHUNKS

    anywhere = pl.BlockSpec(memory_space=pltpu.HBM)
    onchip = pl.BlockSpec(memory_space=pltpu.VMEM)
    dma = pltpu.SemaphoreType.DMA
    scratch = [
        pltpu.VMEM((seq, chans), BF16),
        pltpu.VMEM((seq, chans), BF16),
        pltpu.VMEM((rows, width), BF16),
        pltpu.VMEM(out_proj.shape, BF16),
        pltpu.VMEM((top, 2 * rows), jnp.int32),
        pltpu.VMEM((top, 2 * rows), F32),
        pltpu.VMEM((2, 16, chans), BF16),
        pltpu.VMEM((seq + 16, chans), F32),
        pltpu.VMEM((seq, chans), F32),
        pltpu.VMEM((chans, 4 * chans), F32),
        pltpu.VMEM((seq, chans), F32),
        pltpu.VMEM((seq, chans), F32),
        pltpu.VMEM((seq, chans), F32),
        pltpu.VMEM((seq, chans), F32),
        pltpu.VMEM((n_sp, 8, chans), F32),
        pltpu.VMEM((seq, chans), BF16),
        pltpu.VMEM((rows, n_tp * chans), BF16),
        pltpu.VMEM((rows, width), F32),
        pltpu.VMEM((rows, width), F32),
        pltpu.VMEM((rows, width), BF16),
        pltpu.VMEM((slots, width), BF16),
        pltpu.VMEM((2, slots, width), BF16),
        pltpu.VMEM((nz, hs, width), BF16),
        pltpu.VMEM((nz, hs, width), BF16),
        pltpu.VMEM((2, nz * hs, half), BF16),
        pltpu.VMEM((2, 2 * slots, nz * hs), BF16),
        [pltpu.VMEM((2 * slots, w), BF16) for w in WIDTHS],
        [pltpu.VMEM((2, slots, w), BF16) for w in WIDTHS],
        pltpu.VMEM((2 * rows, slots), BF16),
        pltpu.SemaphoreType.REGULAR((4,)),
        dma((9,)),
        dma((2,)),
        dma((2,)),
        dma((2,)),
        dma((2,)),
        dma((1,)),
        dma((n_sp - 1,)),
        dma((2,)),
        dma((2, nz * hs // min(256, nz * hs))),
        dma((2, nz * hs // min(256, nz * hs))),
        dma((2,)),
        dma((2, pieces, far)),
        dma((2, pieces, far)),
        dma((CHUNKS, 2)),
        dma((CHUNKS, 2)),
    ]
    where = [
        anywhere,
        anywhere,
        onchip,
        onchip,
        onchip,
        onchip,
        onchip,
        onchip,
        onchip,
        anywhere,
        anywhere,
        onchip,
        anywhere,
        anywhere,
        anywhere,
        anywhere,
        anywhere,
    ]
    return pl.pallas_call(
        functools.partial(kernel, n_sp, n_tp),
        out_shape=jax.ShapeDtypeStruct((rows, width), BF16),
        in_specs=where,
        out_specs=onchip,
        scratch_shapes=scratch,
        compiler_params=pltpu.CompilerParams(
            collective_id=0, has_side_effects=True, vmem_limit_bytes=60 * 1024 * 1024
        ),
    )(
        mix_in,
        gate_in,
        conv_w,
        conv_b.reshape(1, chans),
        decay_param,
        recur_gate,
        recur_bias,
        input_gate,
        input_bias,
        residual,
        out_proj,
        norm_gain,
        routes.T,
        route_wt.T,
        exp_gate[0].T,
        exp_up[0].T,
        exp_down[0],
    )


def solution(mesh):
    return jax.shard_map(
        on_device,
        mesh=mesh,
        in_specs=(
            P("sp", "tp"),
            P("sp", "tp"),
            P(None, "tp"),
            P("tp"),
            P(None, "tp"),
            P(None, "tp", None, None),
            P(None, "tp"),
            P(None, "tp", None, None),
            P(None, "tp"),
            P(("sp", "tp"), None),
            P(),
            P(),
            P("sp", None),
            P("sp", None),
            P("sp", None, "tp"),
            P("sp", None, "tp"),
            P("sp", "tp", None),
        ),
        out_specs=P(("sp", "tp"), None),
        check_vma=False,
    )
```
